32 devices in a mesh: ep: 8 (over z, x), tp: 4 (over y, core).
Axes of the slice: x: 2, y: 2, z: 4, core: 2. Of those that a mesh axis runs over, the one named last changes fastest.
Arguments:
- queries: bfloat16 [2048, 1024], P('ep', 'tp'), may hold values from -6 to 6
- key_rows: bfloat16 [2048, 1024], P('ep', 'tp'), may hold values from -6 to 6
- value_rows: bfloat16 [2048, 1024], P('ep', 'tp'), may hold values from -6 to 6
- out_gate: bfloat16 [2048, 1024], P('ep', 'tp'), may hold values from -6 to 6
- log_decay: float32 [2048, 8], P('ep', 'tp'), may hold values from -3 to 0, as said below
- head_gain: float32 [8, 128], P('tp'), may hold values from 0.1 to 1.9
- out_weight: bfloat16 [1024, 2048], P('tp'), may hold values from -0.1875 to 0.1875
- moe_input: bfloat16 [1024, 2048], P('ep'), may hold values from -6 to 6
- moe_gain: float32 [2048], replicated, may hold values from 0.1 to 1.9
- expert_gate: bfloat16 [8, 2048, 3584], P('ep', None, 'tp'), may hold values from -0.125 to 0.125
- expert_up: bfloat16 [8, 2048, 3584], P('ep', None, 'tp'), may hold values from -0.125 to 0.125
- expert_down: bfloat16 [8, 3584, 2048], P('ep', 'tp'), may hold values from -0.125 to 0.125
- route_ids: int32 [1024, 2], P('ep'), may hold values from 0 to 7, all different within a row; in each aligned block of 128 rows (0 to 127, 128 to 255, ...) at most 64 rows name the same one
- route_weights: float32 [1024, 2], P('ep'), may hold values from 0.2 to 1
Outputs:
- mixer_out: bfloat16 [2048, 2048], P(('ep', 'tp'))
- expert_out: bfloat16 [1024, 2048], P('ep', 'tp')
The draws below stay inside these ranges and needn't reach their ends.
Inputs may be any that keep to these rules, and one draw needn't show every extreme that they name: `route_ids`: among the 2 entries of a row no expert repeats. In each aligned block of 128 rows (the rows of one index of ep) no expert is named more than 64 times, a bound that some block reaches. `log_decay`: every entry is negative.
All inputs are finite; a program needn't handle non-finite values.
Results may differ from the reference program's by a relative error of at most 0.017.
Values may be sent and summed in bfloat16 or wider, within the bound.
A program may use at most 64 MiB of HBM per device.

```python
import math
import jax
import jax.numpy as jnp
import numpy as np
from jax import lax

D = 2048
HEADS = 8
HEAD = 128
EFF = 3584
TOP = 2
TOK_DEV = 256
MOE_TOK = 128
TOKENS = 2048
EXPERTS = 8
CAP = 64
MOE_TOTAL = 1024
N_EP = 8
N_TP = 4


def draw_log_decay(key, part):
    streams = jax.random.split(key, 7)
    ranking = jax.random.permutation(streams[0], HEADS)
    fast_heads = ranking < HEADS // 2
    quick = jnp.exp(jax.random.uniform(streams[1], (HEADS,), jnp.float32, jnp.log(3.0), jnp.log(8.0))) / TOK_DEV
    gentle = jnp.exp(jax.random.uniform(streams[2], (HEADS,), jnp.float32, jnp.log(0.03), jnp.log(0.25))) / TOKENS
    fading_speeds = jnp.where(fast_heads, quick, gentle)
    blocks = TOKENS // TOK_DEV
    multiplier_coefficient = jnp.exp(jax.random.uniform(streams[3], (blocks,), jnp.float32, jnp.log(0.5), jnp.log(2.0)))
    multiplier_coefficient = jnp.repeat(multiplier_coefficient, TOK_DEV)
    approximate_guess = jnp.exp(jax.random.uniform(streams[4], (TOKENS, HEADS), jnp.float32, -0.5, 0.5))
    word_slot_spots = jax.random.randint(streams[5], (2, HEADS), 0, TOKENS)
    stack_level_count = jax.random.uniform(streams[6], (2, HEADS), jnp.float32, jnp.log(0.6), jnp.log(0.85))
    sequence_offsets = jnp.arange(TOKENS, dtype=jnp.int32)[:, None, None]
    spike_clusters = jnp.sum(jnp.where(sequence_offsets == word_slot_spots[None], stack_level_count[None], 0.0), axis=1)
    return -(fading_speeds[None, :] * multiplier_coefficient[:, None] * approximate_guess) + spike_clusters


def raised(values, stream_key, source, target, parts, factor):
    owner, partner = [(jnp.arange(values.shape[position]) // (values.shape[position] // parts)).reshape([-1 if axis == position else 1 for axis in range(values.ndim)]) for position in (source, target)]
    chosen = jax.random.permutation(stream_key, parts)[partner]
    strong = (owner == chosen) | (owner == (partner + parts // 2) % parts)
    return jnp.where(strong, factor * values, values)


def levels(stream_key, shape, cuts, low, high):
    level, own = 1.0, jax.random.fold_in(stream_key, 6)
    for position, parts in cuts:
        draws = jnp.exp(jax.random.uniform(jax.random.fold_in(own, position), (parts,), jnp.float32, low / len(cuts), high / len(cuts)))
        level = level * jnp.repeat(draws, shape[position] // parts).reshape([-1 if axis == position else 1 for axis in range(len(shape))])
    return level


def assign_block(key, own, number, rows, amount, top, bound, lean):
    order = jax.random.permutation(key, amount)
    packed, ordinary = load_shares(amount, rows * top, bound, lean, True), load_shares(amount, rows * top, bound, lean, False)
    places = jnp.arange(amount)

    def named(tallies, rotation):
        used = int((tallies > 0).sum())
        fixed = max(1, used // 4)
        passed = fixed + (places - fixed + rotation * (used - fixed)) % max(1, amount - fixed)
        return jnp.zeros((amount,), jnp.int32).at[order[jnp.where(places < fixed, places, passed)]].set(jnp.asarray(tallies, jnp.int32))

    tallies = jnp.where(number % 4 == 0, named(packed, number // 4), named(ordinary, number - number // 4 - 1))
    mixed = jax.random.permutation(jax.random.fold_in(own, 3), amount)
    source_of, sink = mixed[0:amount // 2 * 2:2], mixed[1:amount // 2 * 2:2]
    room = jnp.minimum(tallies[source_of] - 1, bound - tallies[sink]) // 2
    room = jnp.where((source_of == order[0]) | (sink == order[0]) | (tallies[sink] == 0), 0, jnp.maximum(room, 0))
    passed = jax.random.randint(jax.random.fold_in(own, 4), (amount // 2,), 0, 1 << 20) % (room + 1)
    tallies = tallies.at[source_of].add(-passed).at[sink].add(passed)
    members = jnp.searchsorted(jnp.cumsum(tallies), jnp.arange(rows * top), side="right").astype(jnp.int32)
    table = members.reshape(top, rows).T
    table = table[jax.random.permutation(jax.random.fold_in(own, 1), rows)]
    rotation = jax.random.randint(jax.random.fold_in(own, 2), (rows, 1), 0, top)
    return jnp.take_along_axis(table, (jnp.arange(top)[None, :] + rotation) % top, axis=1)


def load_shares(count, total, most, slope, full):
    loads = [(1 << 20) // math.isqrt(grade ** slope) + 1 for grade in range(1, count + 1)]
    largest = most if full else min(most, max(-(-total // count), total * loads[0] // sum(loads)))
    least = 1 if total - largest >= count - 1 else 0
    holding, rest = [largest] + [least] * (count - 1), total - largest - least * (count - 1)
    while rest > 0:
        free = [i for i in range(1, count) if holding[i] < largest] or [i for i in range(1, count) if holding[i] < most]
        mass, left = sum([loads[i] for i in free]), rest
        for i in free:
            more = min(most - holding[i], max(1, left * loads[i] // mass), rest)
            holding[i] = holding[i] + more
            rest = rest - more
    return np.array(holding)


def noise(key, dims, scale, most, cuts=(), kind=jnp.bfloat16):
    drawn = scale * jax.random.normal(key, dims, jnp.float32)
    if cuts:
        drawn = drawn * levels(key, dims, cuts, -0.22, 0.18)
    return jnp.clip(drawn, -most, most).astype(kind)


def noise_with(own_key, shape, width, most, pieces, heavy, held_as=jnp.bfloat16):
    entries = width * jax.random.normal(own_key, shape, jnp.float32)
    if pieces:
        entries = entries * levels(own_key, shape, pieces, -0.22, 0.18)
    return jnp.clip(raised(entries, jax.random.fold_in(own_key, 3), *heavy), -most, most).astype(held_as)


def setup_inputs(seed: int = 0) -> dict:
    streams_of = jax.random.split(jax.random.key(seed), 15)
    queries = noise(streams_of[0], (TOKENS, HEADS * HEAD), 1.0, 6.0, ((0, 8), (1, 4)))
    key_rows = noise(streams_of[1], (TOKENS, HEADS * HEAD), 1.0, 6.0, ((0, 8), (1, 4)))
    value_rows = noise(streams_of[2], (TOKENS, HEADS * HEAD), 1.0, 6.0, ((0, 8), (1, 4)))
    out_gate = noise(streams_of[3], (TOKENS, HEADS * HEAD), 1.0, 6.0, ((0, 8), (1, 4)))
    log_decay = draw_log_decay(jax.random.fold_in(streams_of[14], 71), 0)
    head_gain = jnp.clip(1.0 + 0.18 * jax.random.normal(streams_of[5], (HEADS, HEAD), jnp.float32), 0.1, 1.9)
    out_weight = noise(streams_of[6], (HEADS * HEAD, D), (HEADS * HEAD) ** -0.5, 0.1875, ((0, 4),))
    moe_input = noise(streams_of[7], (MOE_TOTAL, D), 1.0, 6.0, ((0, 8),))
    moe_gain = jnp.clip(1.0 + 0.18 * jax.random.normal(streams_of[8], (D,), jnp.float32), 0.1, 1.9)
    expert_gate = noise(streams_of[9], (EXPERTS, D, EFF), D ** -0.5, 0.125, ((0, 8), (2, 4)))
    expert_up = noise(streams_of[10], (EXPERTS, D, EFF), D ** -0.5, 0.125, ((0, 8), (2, 4)))
    expert_down = noise_with(streams_of[11], (EXPERTS, EFF, D), EFF ** -0.5, 0.125, ((0, 8), (1, 4)), (1, 2, 4, 2.0))
    route_ids_keys = jax.random.split(jax.random.fold_in(streams_of[12], 1), MOE_TOTAL // MOE_TOK)
    route_ids_turns = jax.random.permutation(jax.random.fold_in(streams_of[12], 3), MOE_TOTAL // MOE_TOK)
    route_ids = jax.vmap(lambda own, number: assign_block(jax.random.fold_in(streams_of[12], 2), own, number, MOE_TOK, EXPERTS, TOP, CAP, 2))(route_ids_keys, route_ids_turns).reshape((MOE_TOTAL, TOP))
    route_weights = jnp.clip(0.2 + 0.8 * jax.random.uniform(streams_of[13], (MOE_TOTAL, TOP), jnp.float32) ** levels(streams_of[13], (MOE_TOTAL, TOP), ((0, 8),), -0.2, 0.2), 0.2, 1.0)
    return {"queries": queries, "key_rows": key_rows, "value_rows": value_rows, "out_gate": out_gate, "log_decay": log_decay, "head_gain": head_gain, "out_weight": out_weight, "moe_input": moe_input, "moe_gain": moe_gain, "expert_gate": expert_gate, "expert_up": expert_up, "expert_down": expert_down, "route_ids": route_ids, "route_weights": route_weights}


epsilon = 1e-06

def retention_block(state, inputs):
    query_heads, key_heads, value_heads, decay_block = inputs
    query_f = query_heads.astype(jnp.float32)
    key_f = key_heads.astype(jnp.float32)
    value_f = value_heads.astype(jnp.float32)
    cumulative = jnp.cumsum(decay_block, axis=0)
    block_total = cumulative[-1]
    scores = jnp.einsum('thd,shd->hts', query_f, key_f) * HEAD ** (-0.5)
    level = cumulative.T
    causal = jnp.arange(TOK_DEV, dtype=jnp.int32)[:, None] >= jnp.arange(TOK_DEV, dtype=jnp.int32)[None, :]
    spread = jnp.where(causal[None], level[:, :, None] - level[:, None, :], -jnp.inf)
    weights = (scores * jnp.exp(spread)).astype(jnp.bfloat16)
    inner = jnp.einsum('hts,shd->thd', weights.astype(jnp.float32), value_f)
    carried = jnp.einsum('thd,hde->the', query_f * jnp.exp(cumulative)[:, :, None], state, precision=lax.Precision.HIGHEST)
    scaled_keys = key_f * jnp.exp(block_total[None, :] - cumulative)[:, :, None]
    fresh = jnp.einsum('thd,the->hde', scaled_keys, value_f, precision=lax.Precision.HIGHEST)
    new_state = jnp.exp(block_total)[:, None, None] * state + fresh
    return (new_state, inner + carried)

def retention_ref(queries, key_rows, value_rows, out_gate, log_decay, head_gain, out_weight):
    blocks = TOKENS // TOK_DEV
    shaped = (blocks, TOK_DEV, HEADS, HEAD)
    start = jnp.zeros((HEADS, HEAD, HEAD), jnp.float32)
    _, retained = lax.scan(retention_block, start, (queries.reshape(shaped), key_rows.reshape(shaped), value_rows.reshape(shaped), log_decay.reshape(blocks, TOK_DEV, HEADS)))
    retained = retained.reshape(TOKENS, HEADS, HEAD)
    normed = retained * lax.rsqrt(lax.optimization_barrier(jnp.mean(retained * retained, axis=-1, keepdims=True)) + epsilon) * head_gain[None]
    gated = normed * jax.nn.silu(out_gate.reshape(TOKENS, HEADS, HEAD).astype(jnp.float32))
    heads_out = gated.reshape(TOKENS, HEADS * HEAD).astype(jnp.bfloat16)
    group = HEADS * HEAD // N_TP
    summed = jnp.zeros((TOKENS, D), jnp.float32)
    for member in range(N_TP):
        partial_sum = jnp.dot(heads_out[:, member * group:(member + 1) * group], out_weight[member * group:(member + 1) * group], preferred_element_type=jnp.float32).astype(jnp.bfloat16)
        summed = summed + lax.optimization_barrier(partial_sum).astype(jnp.float32)
    return summed.astype(jnp.bfloat16)

def slot_targets(block_ids):
    flat_ids = block_ids.reshape(-1)
    member = (flat_ids[:, None] == jnp.arange(EXPERTS, dtype=jnp.int32)[None, :]).astype(jnp.int32)
    ranks = lax.optimization_barrier(jnp.sum(jnp.cumsum(member, axis=0) * member, axis=1)) - 1
    return flat_ids * CAP + ranks

def experts_ref(moe_input, moe_gain, expert_gate, expert_up, expert_down, route_ids, route_weights):
    rows_f = moe_input.astype(jnp.float32)
    normed = (rows_f * lax.rsqrt(lax.optimization_barrier(jnp.mean(rows_f * rows_f, axis=-1, keepdims=True)) + epsilon) * moe_gain[None]).astype(jnp.bfloat16)
    pairs = MOE_TOK * TOP
    targets = jax.vmap(slot_targets)(route_ids.reshape(N_EP, MOE_TOK, TOP))
    pair_weights = route_weights.reshape(N_EP, pairs)
    block_index = jnp.arange(N_EP, dtype=jnp.int32)[:, None]
    group = EFF // N_TP

    def one_expert(total, expert):
        wanted = targets // CAP == expert
        local_slot = jnp.where(wanted, targets % CAP, CAP).astype(jnp.int32)
        table = jnp.full((N_EP, CAP + 1), pairs, jnp.int32)
        table = table.at[block_index, local_slot].set(jnp.arange(pairs, dtype=jnp.int32)[None, :])[:, :CAP]
        filled = table < pairs
        pair_index = jnp.minimum(table, pairs - 1)
        token_index = block_index * MOE_TOK + pair_index // TOP
        rows = jnp.where(filled[:, :, None], normed[token_index], jnp.zeros((), jnp.bfloat16)).reshape(N_EP * CAP, D)
        gate_w = lax.dynamic_index_in_dim(expert_gate, expert, 0, keepdims=False)
        up_w = lax.dynamic_index_in_dim(expert_up, expert, 0, keepdims=False)
        down_w = lax.dynamic_index_in_dim(expert_down, expert, 0, keepdims=False)
        hidden = (jax.nn.silu(jnp.dot(rows, gate_w, preferred_element_type=jnp.float32)) * jnp.dot(rows, up_w, preferred_element_type=jnp.float32)).astype(jnp.bfloat16)
        summed = jnp.zeros((N_EP * CAP, D), jnp.float32)
        for member in range(N_TP):
            partial_sum = jnp.dot(hidden[:, member * group:(member + 1) * group], down_w[member * group:(member + 1) * group], preferred_element_type=jnp.float32).astype(jnp.bfloat16)
            summed = summed + lax.optimization_barrier(partial_sum).astype(jnp.float32)
        results = summed.astype(jnp.bfloat16).astype(jnp.float32)
        scale = jnp.where(filled, jnp.take_along_axis(pair_weights, pair_index, axis=1), 0.0)
        contrib = scale.reshape(-1)[:, None] * results
        total = total.at[token_index.reshape(-1)].add(contrib)
        return (total, None)
    start = jnp.zeros((MOE_TOTAL, D), jnp.float32)
    total, _ = lax.scan(one_expert, start, jnp.arange(EXPERTS, dtype=jnp.int32))
    return total.astype(jnp.bfloat16)

def reference(queries, key_rows, value_rows, out_gate, log_decay, head_gain, out_weight, moe_input, moe_gain, expert_gate, expert_up, expert_down, route_ids, route_weights):
    mixer_out = retention_ref(queries, key_rows, value_rows, out_gate, log_decay, head_gain, out_weight)
    expert_out = experts_ref(moe_input, moe_gain, expert_gate, expert_up, expert_down, route_ids, route_weights)
    return (mixer_out, expert_out)
```

```python
import functools

import jax
import jax.numpy as jnp
from jax import lax
from jax.experimental import pallas as pl
from jax.experimental.pallas import tpu as pltpu
from jax.sharding import PartitionSpec as P

epsilon = 1e-06
CHUNKS = 2
PARTS = 2
BF = jnp.bfloat16
F32 = jnp.float32


def dot(a, b, dims=(((1,), (0,)), ((), ()))):
    return lax.dot_general(a, b, dims, preferred_element_type=F32)


def layer_kernel(
    n, cap, heads,
    tok_hbm, ids_hbm, norm_hbm, ld_hbm, k_hbm, v_hbm, q_hbm, rw_hbm, g_hbm, gain_hbm,
    ow_hbm, wg_hbm, wu_hbm, wd_hbm,
    mixer_ref, expert_ref,
    tok_ref, ids_ref, norm_ref, ld_ref, k_ref, v_ref, q_ref, rw_ref, g_ref, gain_ref,
    ow, wg, wu, wd, x, part, near, half, far, done, back,
    st, st_in, tot, tot_in, inner, ho, mx, mr1, ms, mr2,
    w_sem, disp_s, disp_r, st_s, st_r, tot_s, tot_r, fwd_s, fwd_r,
    red_s, red_r, redy_s, redy_r, mix_s, mix_r, ret_s, ret_r,
    piece_ref, hi_ref, lo_ref,
):
    i, j = lax.axis_index("ep"), lax.axis_index("tp")
    j1 = j + 1 - 2 * lax.rem(j, 2)
    j2 = lax.rem(j + 2, 4)
    j3 = lax.rem(j1 + 2, 4)
    places = (j, j1, j2, j3)
    rows = n * cap
    step = rows // CHUNKS
    width = x.shape[2]
    dim = gain_ref.shape[1]
    length = q_ref.shape[0]
    quarter = length // 4

    def shift(p):
        return (p + 1) // 2 if p % 2 else n - p // 2

    def ahead(p):
        return lax.rem(i + shift(p), n)

    def behind(p):
        return lax.rem(i + n - shift(p), n)

    def send(src, dst, ss, rs, dev):
        return pltpu.make_async_remote_copy(
            src_ref=src, dst_ref=dst, send_sem=ss, recv_sem=rs, device_id=dev,
            device_id_type=pl.DeviceIdType.MESH,
        )

    loads = [
        pltpu.make_async_copy(a, b, w_sem.at[m])
        for m, (a, b) in enumerate((
            (tok_hbm, tok_ref), (ids_hbm, ids_ref), (norm_hbm, norm_ref), (ld_hbm, ld_ref),
            (k_hbm, k_ref), (v_hbm, v_ref), (q_hbm, q_ref), (rw_hbm, rw_ref), (g_hbm, g_ref),
            (gain_hbm, gain_ref), (ow_hbm, ow), (wg_hbm, wg), (wu_hbm, wu), (wd_hbm, wd),
        ))
    ]
    for c in loads:
        c.start()
    barrier = pltpu.get_barrier_semaphore()
    for d in range(1, n):
        pl.semaphore_signal(barrier, inc=1, device_id=(ahead(d), j), device_id_type=pl.DeviceIdType.MESH)
    for peer in (j1, j2):
        pl.semaphore_signal(barrier, inc=1, device_id=(i, peer), device_id_type=pl.DeviceIdType.MESH)

    top, tokens = ids_ref.shape
    lanes = -(-n // 16) * 16
    loads[1].wait()
    expert = lax.broadcasted_iota(jnp.int32, (lanes, tokens), 0)
    named = [ids_ref[t : t + 1, :] == expert for t in range(top)]
    strict = lax.broadcasted_iota(jnp.int32, (tokens, tokens), 0) < lax.broadcasted_iota(
        jnp.int32, (tokens, tokens), 1
    )
    held = sum(jnp.where(m, 1.0, 0.0) for m in named)
    before = dot(held.astype(BF), jnp.where(strict, 1.0, 0.0).astype(BF))
    slot = lax.broadcasted_iota(jnp.int32, (rows, tokens), 0)
    target = []
    for t in range(top):
        rank = jnp.sum(jnp.where(named[t], before, 0.0), axis=0, keepdims=True).astype(jnp.int32)
        d = ids_ref[t : t + 1, :] - i
        d = jnp.where(d < 0, d + n, d)
        place = jnp.where(d == 0, 0, jnp.where(2 * d <= n, 2 * d - 1, 2 * (n - d)))
        target.append(place * cap + rank)
    pick = sum(jnp.where(slot == target[t], 1.0, 0.0) for t in range(top)).astype(BF)
    loads[0].wait()
    loads[2].wait()
    rows_f = tok_ref[...].astype(F32)
    scale = lax.rsqrt(jnp.mean(rows_f * rows_f, axis=-1, keepdims=True) + epsilon)
    mine = pl.ds(pl.multiple_of(j * width, width), width)
    normed = (tok_ref[:, mine].astype(F32) * scale * norm_ref[:, mine]).astype(BF)
    piece = dot(pick, normed).astype(BF)
    piece_ref[...] = piece
    x[0, 0:cap, :] = piece[0:cap]
    pl.semaphore_wait(barrier, n + 1)

    sent = []
    disp = [None] * n
    for d in range(1, n):
        r = pl.ds(d * cap, cap)
        disp[d] = send(piece_ref.at[r], x.at[0, r], disp_s.at[d], disp_r.at[d], (ahead(d), j))
        disp[d].start()
        sent.append(disp[d])

    tot[...] = jnp.zeros_like(tot)
    for c in loads[3:10]:
        c.wait()
    comb = sum(jnp.where(slot == target[t], rw_ref[t : t + 1, :], 0.0) for t in range(top)).T
    hi = comb.astype(BF)
    hi_ref[...] = hi
    lo_ref[...] = (comb - hi.astype(F32)).astype(BF)
    causal = lax.broadcasted_iota(jnp.int32, (length, length), 0) >= lax.broadcasted_iota(
        jnp.int32, (length, length), 1
    )
    upper = jnp.where(
        lax.broadcasted_iota(jnp.int32, (length, length), 0)
        <= lax.broadcasted_iota(jnp.int32, (length, length), 1), 1.0, 0.0
    )
    level = lax.dot_general(
        ld_ref[...], upper, (((1,), (0,)), ((), ())),
        precision=lax.Precision.HIGHEST, preferred_element_type=F32,
    )
    cum = [jnp.broadcast_to(level[h : h + 1, :], (dim, length)).T for h in range(heads)]

    for h in range(heads):
        c = slice(h * dim, (h + 1) * dim)
        total = cum[h][length - 1 : length, :]
        keys = k_ref[:, c].astype(F32) * jnp.exp(total - cum[h])
        st[h * dim : (h + 1) * dim, :] = dot(keys.T.astype(BF), v_ref[:, c]).astype(BF)
        tot[h : h + 1, :] = total
    st_c, tot_c = [None] * n, [None] * n
    for d in range(1, n):
        later = (lax.rem(i + d, n), j)
        st_c[d] = send(st, st_in.at[d], st_s.at[d], st_r.at[d], later)
        tot_c[d] = send(tot, tot_in.at[d], tot_s.at[d], tot_r.at[d], later)

    y_c, c0_c, c2_c = [], [], []
    small = step // PARTS
    group = n // (CHUNKS * PARTS)
    for u in range(CHUNKS * PARTS):
        r = pl.ds(u * small, small)
        y_c.append(send(x.at[0, r], x.at[2, r], fwd_s.at[u, 0], fwd_r.at[u, 0], (i, j2)))
        c0_c.append(send(x.at[0, r], x.at[1, r], fwd_s.at[u, 1], fwd_r.at[u, 1], (i, j1)))
        c2_c.append(send(x.at[2, r], x.at[3, r], fwd_s.at[u, 2], fwd_r.at[u, 2], (i, j1)))
    sent += y_c + c0_c + c2_c

    def forward(u):
        for d in range(max(1, u * group), (u + 1) * group):
            disp[d].wait_recv()
        y_c[u].start()
        c0_c[u].start()

    def relay(u):
        y_c[u].wait_recv()
        c2_c[u].start()

    for u in range(PARTS):
        forward(u)
    for d in range(1, n):
        @pl.when(i + d < n)
        def _():
            st_c[d].start()
            tot_c[d].start()

    for h in range(heads):
        c = slice(h * dim, (h + 1) * dim)
        scores = dot(q_ref[:, c], k_ref[:, c], (((1,), (1,)), ((), ()))) * dim ** (-0.5)
        spread = jnp.where(causal, cum[h][:, 0:1] - level[h : h + 1, :], -jnp.inf)
        inner[:, c] = dot((scores * jnp.exp(spread)).astype(BF), v_ref[:, c])

    for u in range(PARTS):
        forward(PARTS + u)
        relay(u)
    for c in loads[10:]:
        c.wait()

    def stripe(m):
        return pl.ds(pl.multiple_of(places[m] * quarter, quarter), quarter)

    mix_a = send(mx.at[stripe(1)], mr1.at[0], mix_s.at[0], mix_r.at[0], (i, j1))
    mix_b = send(mx.at[stripe(3)], mr1.at[1], mix_s.at[1], mix_r.at[1], (i, j1))
    mix_c = send(ms, mr2, mix_s.at[2], mix_r.at[2], (i, j2))
    sent += [mix_a, mix_b, mix_c]

    def retention():
        entering = jnp.zeros((heads * dim, dim), F32)
        for d in range(n - 1, 0, -1):
            @pl.when(i >= d)
            def _():
                st_c[d].wait_recv()
                tot_c[d].wait_recv()

            @pl.when(i < d)
            def _():
                st_in[d] = jnp.zeros(st_in.shape[1:], BF)
                tot_in[d] = jnp.zeros(tot_in.shape[1:], F32)

            decay = jnp.concatenate(
                [jnp.broadcast_to(jnp.exp(tot_in[d, h : h + 1, :]), (dim, dim)) for h in range(heads)], axis=0
            )
            entering = decay * entering + st_in[d].astype(F32)
        entering = entering.astype(BF)
        for h in range(heads):
            c = slice(h * dim, (h + 1) * dim)
            queries = (q_ref[:, c].astype(F32) * jnp.exp(cum[h])).astype(BF)
            kept = inner[:, c] + dot(queries, entering[h * dim : (h + 1) * dim, :])
            normed = kept * lax.rsqrt(jnp.mean(kept * kept, axis=-1, keepdims=True) + epsilon)
            ho[:, c] = (normed * gain_ref[h : h + 1, :] * jax.nn.silu(g_ref[:, c].astype(F32))).astype(BF)
        mx[...] = dot(ho[...], ow[...]).astype(BF)

        mix_b.start()
        mix_a.start()

    red, red_y = [], []
    for g in range(CHUNKS):
        r = pl.ds(g * step, step)
        red.append((
            send(part.at[1, r], near.at[0, r], red_s.at[g, 0], red_r.at[g, 0], (i, j1)),
            send(part.at[3, r], near.at[1, r], red_s.at[g, 1], red_r.at[g, 1], (i, j1)),
        ))
        sent += list(red[-1])
    for u in range(CHUNKS * PARTS):
        r = pl.ds(u * small, small)
        red_y.append(send(half.at[r], far.at[r], redy_s.at[u], redy_r.at[u], (i, j2)))
    sent += red_y

    def block(m):
        return pl.ds(pl.multiple_of(places[m] * width, width), width)

    def experts(g, between):
        r = pl.ds(g * step, step)
        gate, up = 0.0, 0.0
        for m in (0, 2, 1, 3):
            if m == 1:
                for u in range(g * PARTS, (g + 1) * PARTS):
                    c0_c[u].wait_recv()
                    c2_c[u].wait_recv()
            gate = gate + dot(x[m, r, :], wg[block(m), :])
            up = up + dot(x[m, r, :], wu[block(m), :])
        hidden = (jax.nn.silu(gate) * up).astype(BF)
        between()
        for m in (3, 2, 1, 0):
            part[m, r, :] = dot(hidden, wd[:, block(m)]).astype(BF)
            if m == 3:
                red[g][1].start()
            if m == 1:
                red[g][0].start()
                cross(g)

    def cross(g):
        red[g][1].wait_recv()
        for u in range(g * PARTS, (g + 1) * PARTS):
            r = pl.ds(u * small, small)
            half[r, :] = (part[2, r, :].astype(F32) + near[1, r, :].astype(F32)).astype(BF)
            red_y[u].start()

    ret = [None] * n
    for d in range(n):
        r = pl.ds(d * cap, cap)
        if d:
            ret[d] = send(done.at[r], back.at[r], ret_s.at[d], ret_r.at[d], (behind(d), j))
            sent.append(ret[d])

    def home(g):
        red[g][0].wait_recv()
        for u in range(g * PARTS, (g + 1) * PARTS):
            r = pl.ds(u * small, small)
            red_y[u].wait_recv()
            done[r, :] = (
                part[0, r, :].astype(F32) + near[0, r, :].astype(F32) + far[r, :].astype(F32)
            ).astype(BF)
            for d in range(u * group, (u + 1) * group):
                if d:
                    ret[d].start()
                else:
                    back[pl.ds(0, cap), :] = done[pl.ds(0, cap), :]

    def mix_cross():
        mix_b.wait_recv()
        ms[...] = (mx[stripe(2), :].astype(F32) + mr1[1].astype(F32)).astype(BF)
        mix_c.start()

    experts(0, lambda: None)
    for u in range(PARTS, CHUNKS * PARTS):
        relay(u)
    retention()
    for g in range(1, CHUNKS):
        experts(g, mix_cross if g == 1 else lambda: None)
        home(g - 1)
    mix_a.wait_recv()
    mix_c.wait_recv()
    mixer_ref[...] = (
        mx[stripe(0), :].astype(F32) + mr1[0].astype(F32) + mr2[...].astype(F32)
    ).astype(BF)
    home(CHUNKS - 1)
    for d in range(1, n):
        ret[d].wait_recv()
    expert_ref[...] = (dot(hi_ref[...], back[...]) + dot(lo_ref[...], back[...])).astype(BF)
    for c in sent:
        c.wait_send()
    for d in range(1, n):
        @pl.when(i + d < n)
        def _():
            st_c[d].wait_send()
            tot_c[d].wait_send()


def store_kernel(mixer, blended, mixer_out, blended_out, sem):
    copies = [
        pltpu.make_async_copy(mixer, mixer_out, sem.at[0]),
        pltpu.make_async_copy(blended, blended_out, sem.at[1]),
    ]
    for c in copies:
        c.start()
    for c in copies:
        c.wait()


def per_device(
    queries, key_rows, value_rows, out_gate, log_decay, head_gain, out_weight,
    moe_input, moe_gain, expert_gate, expert_up, expert_down, route_ids, route_weights,
):
    n, shares = lax.axis_size("ep"), lax.axis_size("tp")
    tokens, top = route_ids.shape
    pairs = tokens * top
    cap = -(-2 * pairs // n // 16) * 16
    full = moe_input.shape[1]
    width = full // shares
    length, heads = log_decay.shape
    dim = head_gain.shape[1]
    hidden = expert_gate.shape[2]

    rows = n * cap
    quarter = length // shares
    vmem = pl.BlockSpec(memory_space=pltpu.VMEM)
    hbm = pl.BlockSpec(memory_space=pltpu.HBM)
    dma = pltpu.SemaphoreType.DMA
    args = (
        moe_input, route_ids.T, moe_gain.reshape(1, full), log_decay.T, key_rows, value_rows, queries,
        route_weights.T, out_gate, head_gain, out_weight, expert_gate[0], expert_up[0], expert_down[0],
    )
    args = [pltpu.with_memory_space_constraint(a, pltpu.HBM) for a in args]
    mixer, blended = pl.pallas_call(
        functools.partial(layer_kernel, n, cap, heads),
        out_shape=(
            pltpu.VMEM((quarter, full), BF),
            pltpu.VMEM((tokens, width), BF),
        ),
        in_specs=[hbm] * len(args),
        out_specs=(vmem, vmem),
        scratch_shapes=[pltpu.VMEM(a.shape, a.dtype) for a in args[:10]] + [
            pltpu.VMEM(out_weight.shape, BF),
            pltpu.VMEM((full, hidden), BF),
            pltpu.VMEM((full, hidden), BF),
            pltpu.VMEM((hidden, full), BF),
            pltpu.VMEM((4, rows, width), BF),
            pltpu.VMEM((4, rows, width), BF),
            pltpu.VMEM((2, rows, width), BF),
            pltpu.VMEM((rows, width), BF),
            pltpu.VMEM((rows, width), BF),
            pltpu.VMEM((rows, width), BF),
            pltpu.VMEM((rows, width), BF),
            pltpu.VMEM((heads * dim, dim), BF),
            pltpu.VMEM((n, heads * dim, dim), BF),
            pltpu.VMEM((8, dim), F32),
            pltpu.VMEM((n, 8, dim), F32),
            pltpu.VMEM((length, heads * dim), F32),
            pltpu.VMEM((length, heads * dim), BF),
            pltpu.VMEM((length, full), BF),
            pltpu.VMEM((2, quarter, full), BF),
            pltpu.VMEM((quarter, full), BF),
            pltpu.VMEM((quarter, full), BF),
            dma((len(args),)),
            dma((n,)), dma((n,)), dma((n,)), dma((n,)), dma((n,)), dma((n,)),
            dma((CHUNKS * PARTS, 3)), dma((CHUNKS * PARTS, 3)),
            dma((CHUNKS, 2)), dma((CHUNKS, 2)),
            dma((CHUNKS * PARTS,)), dma((CHUNKS * PARTS,)),
            dma((3,)), dma((3,)),
            dma((n,)), dma((n,)),
            pltpu.VMEM((rows, width), BF),
            pltpu.VMEM((tokens, rows), BF),
            pltpu.VMEM((tokens, rows), BF),
        ],
        compiler_params=pltpu.CompilerParams(
            collective_id=0, has_side_effects=True, vmem_limit_bytes=56 * 1024 * 1024
        ),
    )(*args)
    return pl.pallas_call(
        store_kernel,
        out_shape=(
            jax.ShapeDtypeStruct(mixer.shape, BF),
            jax.ShapeDtypeStruct(blended.shape, BF),
        ),
        in_specs=[vmem, vmem],
        out_specs=(hbm, hbm),
        scratch_shapes=[dma((2,))],
        compiler_params=pltpu.CompilerParams(vmem_limit_bytes=4 * 1024 * 1024),
    )(mixer, blended)


def solution(mesh):
    in_specs = (
        P("ep", "tp"),
        P("ep", "tp"),
        P("ep", "tp"),
        P("ep", "tp"),
        P("ep", "tp"),
        P("tp", None),
        P("tp", None),
        P("ep", None),
        P(),
        P("ep", None, "tp"),
        P("ep", None, "tp"),
        P("ep", "tp", None),
        P("ep", None),
        P("ep", None),
    )
    out_specs = (P(("ep", "tp"), None), P("ep", "tp"))
    return jax.shard_map(
        per_device, mesh=mesh, in_specs=in_specs, out_specs=out_specs, check_vma=False
    )
```

```python
import functools

import jax
import jax.numpy as jnp
from jax import lax
from jax.experimental import pallas as pl
from jax.experimental.pallas import tpu as pltpu
from jax.sharding import PartitionSpec as P

epsilon = 1e-06
CHUNKS = 4
PIECES = 8
BF = jnp.bfloat16
F32 = jnp.float32


def dot(a, b, dims=(((1,), (0,)), ((), ()))):
    return lax.dot_general(a, b, dims, preferred_element_type=F32)


def layer_kernel(
    n, cap, heads,
    tok_hbm, ids_hbm, norm_hbm, ld_hbm, k_hbm, v_hbm, q_hbm, rw_hbm, g_hbm, gain_hbm,
    ow_hbm, wg_hbm, wu_hbm, wd_hbm,
    mixer_ref, expert_ref,
    tok_ref, ids_ref, norm_ref, ld_ref, k_ref, v_ref, q_ref, rw_ref, g_ref, gain_ref,
    ow, wg, wu, wd, x, part, near, half, far, done, back,
    st, st_in, tot, tot_in, window, enter, inner, ho, mx, mr1, ms, mr2,
    w_sem, disp_s, disp_r, both_s, both_r, st_s, st_r, tot_s, tot_r, y_s, y_r, c_s, c_r,
    red_s, red_r, redy_s, redy_r, mix_s, mix_r, ret_s, ret_r,
    piece_ref, both_ref, hi_ref, lo_ref,
):
    i, j = lax.axis_index("ep"), lax.axis_index("tp")
    j1 = j + 1 - 2 * lax.rem(j, 2)
    j2 = lax.rem(j + 2, 4)
    j3 = lax.rem(j1 + 2, 4)
    places = (j, j1, j2, j3)
    rows = n * cap
    step = rows // CHUNKS
    small = rows // PIECES
    width = x.shape[2]
    dim = gain_ref.shape[1]
    length = q_ref.shape[0]
    quarter = length // 4
    rounds = n.bit_length() - 1

    def partner(d):
        r = i
        for b in range(rounds):
            if (d >> b) & 1:
                r = r + (1 << b) * (1 - 2 * lax.rem(lax.div(i, 1 << b), 2))
        return r

    def position(d):
        return (((d >> 1) & 1) * 2 + d // (n // 2)) * (n // 4) + ((d % (n // 2)) >> 2) * 2 + (d & 1)

    offsets = sorted(range(n), key=position)

    def members(p):
        return [d for d in offsets[p * n // PIECES : (p + 1) * n // PIECES]]

    def slots(d):
        return pl.ds(position(d) * cap, cap)

    def chunk(g):
        return pl.ds(g * step, step)

    def bit(p):
        return pl.ds(p * small, small)

    def of(g):
        return range(g * PIECES // CHUNKS, (g + 1) * PIECES // CHUNKS)

    def across(g):
        return g % 2 == 1

    def send(src, dst, ss, rs, dev):
        return pltpu.make_async_remote_copy(
            src_ref=src, dst_ref=dst, send_sem=ss, recv_sem=rs, device_id=dev,
            device_id_type=pl.DeviceIdType.MESH,
        )

    loads = [
        pltpu.make_async_copy(a, b, w_sem.at[m])
        for m, (a, b) in enumerate((
            (tok_hbm, tok_ref), (ids_hbm, ids_ref), (norm_hbm, norm_ref), (ld_hbm, ld_ref),
            (k_hbm, k_ref), (v_hbm, v_ref), (q_hbm, q_ref), (rw_hbm, rw_ref), (g_hbm, g_ref),
            (gain_hbm, gain_ref), (ow_hbm, ow), (wg_hbm, wg), (wu_hbm, wu), (wd_hbm, wd),
        ))
    ]
    for c in loads:
        c.start()
    barrier = pltpu.get_barrier_semaphore()
    for d in range(1, n):
        pl.semaphore_signal(barrier, inc=1, device_id=(partner(d), j), device_id_type=pl.DeviceIdType.MESH)
    for peer in (j1, j2):
        pl.semaphore_signal(barrier, inc=1, device_id=(i, peer), device_id_type=pl.DeviceIdType.MESH)

    def block(m):
        return pl.ds(pl.multiple_of(places[m] * width, width), width)

    top, tokens = ids_ref.shape
    lanes = -(-n // 16) * 16
    loads[1].wait()
    expert = lax.broadcasted_iota(jnp.int32, (lanes, tokens), 0)
    named = [ids_ref[t : t + 1, :] == expert for t in range(top)]
    strict = lax.broadcasted_iota(jnp.int32, (tokens, tokens), 0) < lax.broadcasted_iota(
        jnp.int32, (tokens, tokens), 1
    )
    held = sum(jnp.where(m, 1.0, 0.0) for m in named)
    before = dot(held.astype(BF), jnp.where(strict, 1.0, 0.0).astype(BF))
    slot = lax.broadcasted_iota(jnp.int32, (rows, tokens), 0)
    target = []
    for t in range(top):
        rank = jnp.sum(jnp.where(named[t], before, 0.0), axis=0, keepdims=True).astype(jnp.int32)
        d = jnp.bitwise_xor(ids_ref[t : t + 1, :], i)
        over = jnp.where(d >= n // 2, 1, 0)
        kept = d - over * (n // 2)
        place = ((d >> 1) & 1) * 2 + over
        place = place * (n // 4) + (kept >> 2) * 2 + (d & 1)
        target.append(place * cap + rank)
    pick = sum(jnp.where(slot == target[t], 1.0, 0.0) for t in range(top)).astype(BF)
    loads[0].wait()
    loads[2].wait()
    rows_f = tok_ref[...].astype(F32)
    scale = lax.rsqrt(jnp.mean(rows_f * rows_f, axis=-1, keepdims=True) + epsilon)

    def normed(m):
        return (tok_ref[:, block(m)].astype(F32) * scale * norm_ref[:, block(m)]).astype(BF)

    piece = dot(pick, normed(0)).astype(BF)
    piece_ref[...] = piece
    x[0, 0:cap, :] = piece[0:cap]
    both = normed(2)
    for g in range(0, CHUNKS, 2):
        both_ref[chunk(g), :] = dot(pick[g * step : (g + 1) * step], both).astype(BF)
    x[2, 0:cap, :] = both_ref[0:cap, :]
    pl.semaphore_wait(barrier, n + 1)

    sent = []
    disp, disp2 = [None] * n, [None] * n
    for d in range(1, n):
        disp[d] = send(piece_ref.at[slots(d)], x.at[0, slots(d)], disp_s.at[d], disp_r.at[d], (partner(d), j))
        sent.append(disp[d])
        if d < n // 2:
            disp2[d] = send(both_ref.at[slots(d)], x.at[2, slots(d)], both_s.at[d], both_r.at[d], (partner(d), j))
            sent.append(disp2[d])

    def dispatch(g):
        for p in of(g):
            for d in members(p):
                if d:
                    disp[d].start()
                    if not across(g):
                        disp2[d].start()

    dispatch(1)
    dispatch(0)

    y_c, c0_c, c2_c = [], [], []
    for p in range(PIECES):
        r = bit(p)
        y_c.append(send(x.at[0, r], x.at[2, r], y_s.at[p], y_r.at[p], (i, j2)))
        c0_c.append(send(x.at[0, r], x.at[1, r], c_s.at[p, 0], c_r.at[p, 0], (i, j1)))
        c2_c.append(send(x.at[2, r], x.at[3, r], c_s.at[p, 1], c_r.at[p, 1], (i, j1)))
        sent += [c0_c[p], c2_c[p]]
        if across(p * CHUNKS // PIECES):
            sent.append(y_c[p])

    def forward(g, which=None):
        for p in of(g) if which is None else [of(g)[which]]:
            for d in members(p):
                if d:
                    disp[d].wait_recv()
                    if not across(g):
                        disp2[d].wait_recv()
            if across(g):
                y_c[p].start()
            else:
                c2_c[p].start()
            c0_c[p].start()

    def relay(g):
        for p in of(g):
            y_c[p].wait_recv()
            c2_c[p].start()

    causal = lax.broadcasted_iota(jnp.int32, (length, length), 0) >= lax.broadcasted_iota(
        jnp.int32, (length, length), 1
    )
    upper = jnp.where(
        lax.broadcasted_iota(jnp.int32, (length, length), 0)
        <= lax.broadcasted_iota(jnp.int32, (length, length), 1), 1.0, 0.0
    )
    for c in loads[3:10]:
        c.wait()
    level = lax.dot_general(
        ld_ref[...], upper, (((1,), (0,)), ((), ())),
        precision=lax.Precision.HIGHEST, preferred_element_type=F32,
    )
    cum = [jnp.broadcast_to(level[h : h + 1, :], (dim, length)).T for h in range(heads)]
    tot[0] = jnp.zeros(tot.shape[1:], F32)
    for h in range(heads):
        c = slice(h * dim, (h + 1) * dim)
        total = cum[h][length - 1 : length, :]
        keys = k_ref[:, c].astype(F32) * jnp.exp(total - cum[h])
        window[c, :] = dot(keys.T.astype(BF), v_ref[:, c])
        tot[0, h : h + 1, :] = total
    st[0] = window[...].astype(BF)
    enter[...] = jnp.zeros_like(enter)
    st_c, tot_c = [], []
    for r in range(rounds):
        later = (lax.rem(i + (1 << r), n), j)
        st_c.append(send(st.at[r], st_in.at[r], st_s.at[r], st_r.at[r], later))
        tot_c.append(send(tot.at[r], tot_in.at[r], tot_s.at[r], tot_r.at[r], later))

    def pass_on(r):
        @pl.when(i + (1 << r) < n)
        def _():
            st_c[r].start()
            tot_c[r].start()

    span = [jnp.zeros(tot.shape[1:], F32)]

    def spread_rows(totals):
        return jnp.concatenate(
            [jnp.broadcast_to(jnp.exp(totals[h : h + 1, :]), (dim, dim)) for h in range(heads)], axis=0
        )

    def absorb(r):
        @pl.when(i >= 1 << r)
        def _():
            st_c[r].wait_recv()
            tot_c[r].wait_recv()

        @pl.when(i < 1 << r)
        def _():
            st_in[r] = jnp.zeros(st_in.shape[1:], BF)
            tot_in[r] = jnp.zeros(tot_in.shape[1:], F32)

        arrived = st_in[r].astype(F32)
        enter[...] = spread_rows(span[0]) * arrived + enter[...]
        span[0] = span[0] + tot_in[r]
        if r + 1 < rounds:
            window[...] = spread_rows(tot[r]) * arrived + window[...]
            st[r + 1] = window[...].astype(BF)
            tot[r + 1] = tot[r] + tot_in[r]
            pass_on(r + 1)

    pass_on(0)
    dispatch(2)
    dispatch(3)

    for h in range(heads):
        c = slice(h * dim, (h + 1) * dim)
        scores = dot(q_ref[:, c], k_ref[:, c], (((1,), (1,)), ((), ()))) * dim ** (-0.5)
        spread = jnp.where(causal, cum[h][:, 0:1] - level[h : h + 1, :], -jnp.inf)
        inner[:, c] = dot((scores * jnp.exp(spread)).astype(BF), v_ref[:, c])

    def stripe(m):
        return pl.ds(pl.multiple_of(places[m] * quarter, quarter), quarter)

    mix_a = send(mx.at[stripe(1)], mr1.at[0], mix_s.at[0], mix_r.at[0], (i, j1))
    mix_b = send(mx.at[stripe(3)], mr1.at[1], mix_s.at[1], mix_r.at[1], (i, j1))
    mix_c = send(ms, mr2, mix_s.at[2], mix_r.at[2], (i, j2))
    sent += [mix_a, mix_b, mix_c]

    def retention():
        entering = enter[...].astype(BF)
        for h in range(heads):
            c = slice(h * dim, (h + 1) * dim)
            queries = (q_ref[:, c].astype(F32) * jnp.exp(cum[h])).astype(BF)
            kept = inner[:, c] + dot(queries, entering[h * dim : (h + 1) * dim, :])
            unit = kept * lax.rsqrt(jnp.mean(kept * kept, axis=-1, keepdims=True) + epsilon)
            ho[:, c] = (unit * gain_ref[h : h + 1, :] * jax.nn.silu(g_ref[:, c].astype(F32))).astype(BF)
        mx[...] = dot(ho[...], ow[...]).astype(BF)
        mix_b.start()
        mix_a.start()

    def mix_cross():
        mix_b.wait_recv()
        ms[...] = (mx[stripe(2), :].astype(F32) + mr1[1].astype(F32)).astype(BF)

    red, red_y = [], []
    for g in range(CHUNKS):
        r = chunk(g)
        red.append((
            send(part.at[1, r], near.at[0, r], red_s.at[g, 0], red_r.at[g, 0], (i, j1)),
            send(part.at[3, r], near.at[1, r], red_s.at[g, 1], red_r.at[g, 1], (i, j1)),
        ))
        sent += list(red[-1])
    for p in range(PIECES):
        r = bit(p)
        red_y.append(send(half.at[r], far.at[r], redy_s.at[p], redy_r.at[p], (i, j2)))
    sent += red_y

    def experts(g, between=None, after=None):
        r = chunk(g)
        gate, up = 0.0, 0.0
        for m in (0, 2, 1, 3):
            if m == 1:
                if between is not None:
                    between()
                for p in of(g):
                    c0_c[p].wait_recv()
                    c2_c[p].wait_recv()
            gate = gate + dot(x[m, r, :], wg[block(m), :])
            up = up + dot(x[m, r, :], wu[block(m), :])
        hidden = (jax.nn.silu(gate) * up).astype(BF)
        if after is not None:
            after()
        for m in (3, 1, 2, 0):
            part[m, r, :] = dot(hidden, wd[:, block(m)]).astype(BF)
            if m == 3:
                red[g][1].start()
            if m == 1:
                red[g][0].start()
        cross(g)

    def cross(g):
        red[g][1].wait_recv()
        for p in of(g):
            r = bit(p)
            half[r, :] = (part[2, r, :].astype(F32) + near[1, r, :].astype(F32)).astype(BF)
            red_y[p].start()

    ret = [None] * n
    for d in range(1, n):
        ret[d] = send(done.at[slots(d)], back.at[slots(d)], ret_s.at[d], ret_r.at[d], (partner(d), j))
        sent.append(ret[d])

    def home(g, which=None):
        if not which:
            red[g][0].wait_recv()
        for p in of(g) if which is None else [of(g)[which]]:
            r = bit(p)
            red_y[p].wait_recv()
            done[r, :] = (
                part[0, r, :].astype(F32) + near[0, r, :].astype(F32) + far[r, :].astype(F32)
            ).astype(BF)
            for d in members(p):
                if d:
                    ret[d].start()
                else:
                    back[0:cap, :] = done[0:cap, :]

    forward(0)
    for c in loads[10:]:
        c.wait()
    experts(0, after=lambda: forward(1))
    absorb(0)
    comb = sum(jnp.where(slot == target[t], rw_ref[t : t + 1, :], 0.0) for t in range(top)).T
    hi = comb.astype(BF)
    hi_ref[...] = hi
    lo_ref[...] = (comb - hi.astype(F32)).astype(BF)
    forward(2)
    relay(1)
    forward(3, 0)
    experts(1, after=lambda: forward(3, 1))
    for r in range(1, rounds - 1):
        absorb(r)
    experts(2)
    home(0)
    relay(3)
    experts(3, after=lambda: home(1, 0))
    home(1, 1)
    absorb(rounds - 1)
    retention()
    home(2)
    home(3, 0)
    mix_cross()
    mix_c.start()
    home(3, 1)

    def gather(g):
        for p in of(g):
            for d in members(p):
                if d:
                    ret[d].wait_recv()
        c = slice(g * step, (g + 1) * step)
        return dot(hi_ref[:, c], back[c, :]) + dot(lo_ref[:, c], back[c, :])

    blend = gather(0) + gather(2) + gather(1)
    mix_a.wait_recv()
    mix_c.wait_recv()
    mixer_ref[...] = (
        mx[stripe(0), :].astype(F32) + mr1[0].astype(F32) + mr2[...].astype(F32)
    ).astype(BF)
    expert_ref[...] = (blend + gather(3)).astype(BF)
    for c in sent:
        c.wait_send()
    for r in range(rounds):
        @pl.when(i + (1 << r) < n)
        def _():
            st_c[r].wait_send()
            tot_c[r].wait_send()


def store_kernel(mixer, blended, mixer_out, blended_out, sem):
    copies = [
        pltpu.make_async_copy(mixer, mixer_out, sem.at[0]),
        pltpu.make_async_copy(blended, blended_out, sem.at[1]),
    ]
    for c in copies:
        c.start()
    for c in copies:
        c.wait()


def per_device(
    queries, key_rows, value_rows, out_gate, log_decay, head_gain, out_weight,
    moe_input, moe_gain, expert_gate, expert_up, expert_down, route_ids, route_weights,
):
    n, shares = lax.axis_size("ep"), lax.axis_size("tp")
    tokens, top = route_ids.shape
    pairs = tokens * top
    cap = -(-2 * pairs // n // 16) * 16
    full = moe_input.shape[1]
    width = full // shares
    length, heads = log_decay.shape
    dim = head_gain.shape[1]
    hidden = expert_gate.shape[2]

    rows = n * cap
    rounds = n.bit_length() - 1
    quarter = length // shares
    vmem = pl.BlockSpec(memory_space=pltpu.VMEM)
    hbm = pl.BlockSpec(memory_space=pltpu.HBM)
    dma = pltpu.SemaphoreType.DMA
    args = (
        moe_input, route_ids.T, moe_gain.reshape(1, full), log_decay.T, key_rows, value_rows, queries,
        route_weights.T, out_gate, head_gain, out_weight, expert_gate[0], expert_up[0], expert_down[0],
    )
    args = [pltpu.with_memory_space_constraint(a, pltpu.HBM) for a in args]
    mixer, blended = pl.pallas_call(
        functools.partial(layer_kernel, n, cap, heads),
        out_shape=(
            pltpu.VMEM((quarter, full), BF),
            pltpu.VMEM((tokens, width), BF),
        ),
        in_specs=[hbm] * len(args),
        out_specs=(vmem, vmem),
        scratch_shapes=[pltpu.VMEM(a.shape, a.dtype) for a in args[:10]] + [
            pltpu.VMEM(out_weight.shape, BF),
            pltpu.VMEM((full, hidden), BF),
            pltpu.VMEM((full, hidden), BF),
            pltpu.VMEM((hidden, full), BF),
            pltpu.VMEM((4, rows, width), BF),
            pltpu.VMEM((4, rows, width), BF),
            pltpu.VMEM((2, rows, width), BF),
            pltpu.VMEM((rows, width), BF),
            pltpu.VMEM((rows, width), BF),
            pltpu.VMEM((rows, width), BF),
            pltpu.VMEM((rows, width), BF),
            pltpu.VMEM((rounds, heads * dim, dim), BF),
            pltpu.VMEM((rounds, heads * dim, dim), BF),
            pltpu.VMEM((rounds, 8, dim), F32),
            pltpu.VMEM((rounds, 8, dim), F32),
            pltpu.VMEM((heads * dim, dim), F32),
            pltpu.VMEM((heads * dim, dim), F32),
            pltpu.VMEM((length, heads * dim), F32),
            pltpu.VMEM((length, heads * dim), BF),
            pltpu.VMEM((length, full), BF),
            pltpu.VMEM((2, quarter, full), BF),
            pltpu.VMEM((quarter, full), BF),
            pltpu.VMEM((quarter, full), BF),
            dma((len(args),)),
            dma((n,)), dma((n,)), dma((n,)), dma((n,)),
            dma((rounds,)), dma((rounds,)), dma((rounds,)), dma((rounds,)),
            dma((PIECES,)), dma((PIECES,)), dma((PIECES, 2)), dma((PIECES, 2)),
            dma((CHUNKS, 2)), dma((CHUNKS, 2)),
            dma((PIECES,)), dma((PIECES,)),
            dma((3,)), dma((3,)),
            dma((n,)), dma((n,)),
            pltpu.VMEM((rows, width), BF),
            pltpu.VMEM((rows, width), BF),
            pltpu.VMEM((tokens, rows), BF),
            pltpu.VMEM((tokens, rows), BF),
        ],
        compiler_params=pltpu.CompilerParams(
            collective_id=0, has_side_effects=True, vmem_limit_bytes=56 * 1024 * 1024
        ),
    )(*args)
    return pl.pallas_call(
        store_kernel,
        out_shape=(
            jax.ShapeDtypeStruct(mixer.shape, BF),
            jax.ShapeDtypeStruct(blended.shape, BF),
        ),
        in_specs=[vmem, vmem],
        out_specs=(hbm, hbm),
        scratch_shapes=[dma((2,))],
        compiler_params=pltpu.CompilerParams(vmem_limit_bytes=4 * 1024 * 1024),
    )(mixer, blended)


def solution(mesh):
    in_specs = (
        P("ep", "tp"),
        P("ep", "tp"),
        P("ep", "tp"),
        P("ep", "tp"),
        P("ep", "tp"),
        P("tp", None),
        P("tp", None),
        P("ep", None),
        P(),
        P("ep", None, "tp"),
        P("ep", None, "tp"),
        P("ep", "tp", None),
        P("ep", None),
        P("ep", None),
    )
    out_specs = (P(("ep", "tp"), None), P("ep", "tp"))
    return jax.shard_map(
        per_device, mesh=mesh, in_specs=in_specs, out_specs=out_specs, check_vma=False
    )
```

```python
import functools

import jax
import jax.numpy as jnp
from jax import lax
from jax.experimental import pallas as pl
from jax.experimental.pallas import tpu as pltpu
from jax.sharding import PartitionSpec as P

epsilon = 1e-06
CHUNKS = 4
PIECES = 8
BF = jnp.bfloat16
F32 = jnp.float32


def dot(a, b, dims=(((1,), (0,)), ((), ()))):
    return lax.dot_general(a, b, dims, preferred_element_type=F32)


def layer_kernel(
    n, cap, heads,
    tok_hbm, ids_hbm, norm_hbm, ld_hbm, rw_hbm, gain_hbm, k_hbm, v_hbm, q_hbm, g_hbm,
    ow_hbm, wg_hbm, wu_hbm, wd_hbm,
    mixer_ref, expert_ref,
    tok_ref, ids_ref, norm_ref, ld_ref, rw_ref, gain_ref, kvqg,
    ow, wg, wu, wd, x, part, near, half, far, done, back,
    st, st_in, tot, tot_in, window, enter, inner, ho, mx, mr1, ms, mr2,
    w_sem, sent_s, disp_r, st_s, st_r, tot_s, tot_r, y_r, c_r, red_r, redy_r, mix_r, ret_r,
    piece_ref, both_ref, hi_ref, lo_ref,
):
    i, j = lax.axis_index("ep"), lax.axis_index("tp")
    j1 = j + 1 - 2 * lax.rem(j, 2)
    j2 = lax.rem(j + 2, 4)
    j3 = lax.rem(j1 + 2, 4)
    places = (j, j1, j2, j3)
    rows = n * cap
    step = rows // CHUNKS
    small = rows // PIECES
    width = x.shape[2]
    dim = gain_ref.shape[1]
    k_ref, v_ref, q_ref, g_ref = [kvqg.at[m] for m in range(4)]
    length = kvqg.shape[1]
    quarter = length // 4
    rounds = n.bit_length() - 1

    def partner(d):
        r = i
        for b in range(rounds):
            if (d >> b) & 1:
                r = r + (1 << b) * (1 - 2 * lax.rem(lax.div(i, 1 << b), 2))
        return r

    def position(d):
        return (((d >> 1) & 1) * 2 + d // (n // 2)) * (n // 4) + ((d % (n // 2)) >> 2) * 2 + (d & 1)

    offsets = sorted(range(n), key=position)

    def members(p):
        return [d for d in offsets[p * n // PIECES : (p + 1) * n // PIECES]]

    def slots(d):
        return pl.ds(position(d) * cap, cap)

    def chunk(g):
        return pl.ds(g * step, step)

    def bit(p):
        return pl.ds(p * small, small)

    def of(g):
        return range(g * PIECES // CHUNKS, (g + 1) * PIECES // CHUNKS)

    def across(g):
        return g % 2 == 1

    def send(src, dst, ss, rs, dev):
        return pltpu.make_async_remote_copy(
            src_ref=src, dst_ref=dst, send_sem=ss, recv_sem=rs, device_id=dev,
            device_id_type=pl.DeviceIdType.MESH,
        )

    DISPATCH, BOTH, ACROSS, CORE, HALVES, SUMS, MIX, HOME = range(8)
    small_loads = [
        pltpu.make_async_copy(a, b, w_sem.at[m])
        for m, (a, b) in enumerate((
            (tok_hbm, tok_ref), (ids_hbm, ids_ref), (norm_hbm, norm_ref), (ld_hbm, ld_ref),
            (rw_hbm, rw_ref), (gain_hbm, gain_ref),
        ))
    ]
    head_loads = [
        pltpu.make_async_copy(a, kvqg.at[m], w_sem.at[6]) for m, a in enumerate((k_hbm, v_hbm, q_hbm, g_hbm))
    ]
    weight_loads = [
        pltpu.make_async_copy(a, b, w_sem.at[7 + m])
        for m, (a, b) in enumerate(((ow_hbm, ow), (wg_hbm, wg), (wu_hbm, wu), (wd_hbm, wd)))
    ]
    for c in small_loads + head_loads + weight_loads:
        c.start()
    barrier = pltpu.get_barrier_semaphore()
    for d in range(1, n):
        pl.semaphore_signal(barrier, inc=1, device_id=(partner(d), j), device_id_type=pl.DeviceIdType.MESH)
    for peer in (j1, j2):
        pl.semaphore_signal(barrier, inc=1, device_id=(i, peer), device_id_type=pl.DeviceIdType.MESH)

    def block(m):
        return pl.ds(pl.multiple_of(places[m] * width, width), width)

    top, tokens = ids_ref.shape
    lanes = -(-n // 16) * 16
    small_loads[1].wait()
    expert = lax.broadcasted_iota(jnp.int32, (lanes, tokens), 0)
    named = [ids_ref[t : t + 1, :] == expert for t in range(top)]
    strict = lax.broadcasted_iota(jnp.int32, (tokens, tokens), 0) < lax.broadcasted_iota(
        jnp.int32, (tokens, tokens), 1
    )
    held = sum(jnp.where(m, 1.0, 0.0) for m in named)
    before = dot(held.astype(BF), jnp.where(strict, 1.0, 0.0).astype(BF))
    slot = lax.broadcasted_iota(jnp.int32, (rows, tokens), 0)
    target = []
    for t in range(top):
        rank = jnp.sum(jnp.where(named[t], before, 0.0), axis=0, keepdims=True).astype(jnp.int32)
        d = jnp.bitwise_xor(ids_ref[t : t + 1, :], i)
        over = jnp.where(d >= n // 2, 1, 0)
        kept = d - over * (n // 2)
        place = ((d >> 1) & 1) * 2 + over
        place = place * (n // 4) + (kept >> 2) * 2 + (d & 1)
        target.append(place * cap + rank)
    pick = sum(jnp.where(slot == target[t], 1.0, 0.0) for t in range(top)).astype(BF)
    small_loads[0].wait()
    small_loads[2].wait()
    rows_f = tok_ref[...].astype(F32)
    scale = lax.rsqrt(jnp.mean(rows_f * rows_f, axis=-1, keepdims=True) + epsilon)

    def normed(m):
        return (tok_ref[:, block(m)].astype(F32) * scale * norm_ref[:, block(m)]).astype(BF)

    piece = dot(pick, normed(0)).astype(BF)
    piece_ref[...] = piece
    x[0, 0:cap, :] = piece[0:cap]
    pl.semaphore_wait(barrier, n + 1)

    def count(r):
        return x.at[0, pl.ds(0, r)]

    disp, disp2 = [None] * n, [None] * n
    for d in range(1, n):
        to = (partner(d), j)
        disp[d] = send(piece_ref.at[slots(d)], x.at[0, slots(d)], sent_s.at[DISPATCH], disp_r.at[d - 1], to)
        if d < n // 2:
            disp2[d] = send(both_ref.at[slots(d)], x.at[2, slots(d)], sent_s.at[BOTH], disp_r.at[d - 1], to)

    def dispatch(g, which=None):
        for p in of(g) if which is None else [of(g)[which]]:
            for d in members(p):
                if d:
                    disp[d].start()
                    if not across(g):
                        disp2[d].start()

    def dispatched(d):
        rows_in = cap if d >= n // 2 else 2 * cap
        send(count(rows_in), count(rows_in), sent_s.at[DISPATCH], disp_r.at[d - 1], (partner(d), j)).wait_recv()

    dispatch(1, 0)
    both = normed(2)
    for g in range(0, CHUNKS, 2):
        both_ref[chunk(g), :] = dot(pick[g * step : (g + 1) * step], both).astype(BF)
    x[2, 0:cap, :] = both_ref[0:cap, :]
    dispatch(0)
    dispatch(1, 1)

    pieces_across = [p for p in range(PIECES) if across(p * CHUNKS // PIECES)]
    y_c, c0_c, c2_c = [None] * PIECES, [], []
    for p in range(PIECES):
        r, g = bit(p), p * CHUNKS // PIECES
        first = 3 * (g // 2) + (1 if across(g) else 0)
        if across(g):
            y_c[p] = send(
                x.at[0, r], x.at[2, r], sent_s.at[ACROSS], y_r.at[pieces_across.index(p)], (i, j2)
            )
        c0_c.append(send(x.at[0, r], x.at[1, r], sent_s.at[CORE], c_r.at[first], (i, j1)))
        c2_c.append(send(x.at[2, r], x.at[3, r], sent_s.at[CORE], c_r.at[first + across(g)], (i, j1)))

    def arrive(g, which=0):
        first = 3 * (g // 2) + (1 + which if across(g) else 0)
        rows_in = step if across(g) else 2 * step
        send(count(rows_in), count(rows_in), sent_s.at[CORE], c_r.at[first], (i, j1)).wait_recv()

    def forward(g, which=None):
        for p in of(g) if which is None else [of(g)[which]]:
            for d in members(p):
                if d:
                    dispatched(d)
            if across(g):
                y_c[p].start()
            else:
                c2_c[p].start()
            c0_c[p].start()

    def relay(g, which=None):
        for p in of(g) if which is None else [of(g)[which]]:
            y_c[p].wait_recv()
            c2_c[p].start()

    causal = lax.broadcasted_iota(jnp.int32, (length, length), 0) >= lax.broadcasted_iota(
        jnp.int32, (length, length), 1
    )
    upper = jnp.where(
        lax.broadcasted_iota(jnp.int32, (length, length), 0)
        <= lax.broadcasted_iota(jnp.int32, (length, length), 1), 1.0, 0.0
    )
    for c in small_loads[3:]:
        c.wait()
    pltpu.make_async_copy(kvqg, kvqg, w_sem.at[6]).wait()
    level = lax.dot_general(
        ld_ref[...], upper, (((1,), (0,)), ((), ())),
        precision=lax.Precision.HIGHEST, preferred_element_type=F32,
    )
    cum = [jnp.broadcast_to(level[h : h + 1, :], (dim, length)).T for h in range(heads)]
    tot[0] = jnp.zeros(tot.shape[1:], F32)
    for h in range(heads):
        c = slice(h * dim, (h + 1) * dim)
        total = cum[h][length - 1 : length, :]
        keys = k_ref[:, c].astype(F32) * jnp.exp(total - cum[h])
        window[c, :] = dot(keys.T.astype(BF), v_ref[:, c])
        tot[0, h : h + 1, :] = total
    st[0] = window[...].astype(BF)
    enter[...] = jnp.zeros_like(enter)
    st_c, tot_c = [], []
    for r in range(rounds):
        later = (lax.rem(i + (1 << r), n) if r else partner(1), j)
        st_c.append(send(st.at[r], st_in.at[r], st_s.at[r], st_r.at[r], later))
        tot_c.append(send(tot.at[r], tot_in.at[r], tot_s.at[r], tot_r.at[r], later))

    second = lax.rem(i, 2) == 1

    def pass_on(r):
        @pl.when(i + (1 << r) < n)
        def _():
            st_c[r].start()
            tot_c[r].start()

    span = [jnp.zeros(tot.shape[1:], F32)]

    def spread_rows(totals):
        return jnp.concatenate(
            [jnp.broadcast_to(jnp.exp(totals[h : h + 1, :]), (dim, dim)) for h in range(heads)], axis=0
        )

    def pair():
        st_c[0].wait_recv()
        tot_c[0].wait_recv()
        own, arrived = window[...], st_in[0].astype(F32)
        late = spread_rows(jnp.where(second, tot[0], tot_in[0]))
        window[...] = late * jnp.where(second, arrived, own) + jnp.where(second, own, arrived)
        st[1] = window[...].astype(BF)
        tot[1] = tot[0] + tot_in[0]
        pass_on(1)

    def absorb(r):
        @pl.when(i >= 1 << r)
        def _():
            st_c[r].wait_recv()
            tot_c[r].wait_recv()

        @pl.when(i < 1 << r)
        def _():
            st_in[r] = jnp.zeros(st_in.shape[1:], BF)
            tot_in[r] = jnp.zeros(tot_in.shape[1:], F32)

        arrived = st_in[r].astype(F32)
        enter[...] = spread_rows(span[0]) * arrived + enter[...]
        span[0] = span[0] + tot_in[r]
        if r + 1 < rounds:
            window[...] = spread_rows(tot[r]) * arrived + window[...]
            st[r + 1] = window[...].astype(BF)
            tot[r + 1] = tot[r] + tot_in[r]
            pass_on(r + 1)

    st_c[0].start()
    tot_c[0].start()
    dispatch(2)
    dispatch(3)

    for h in range(heads):
        c = slice(h * dim, (h + 1) * dim)
        scores = dot(q_ref[:, c], k_ref[:, c], (((1,), (1,)), ((), ()))) * dim ** (-0.5)
        spread = jnp.where(causal, cum[h][:, 0:1] - level[h : h + 1, :], -jnp.inf)
        inner[:, c] = dot((scores * jnp.exp(spread)).astype(BF), v_ref[:, c])

    def stripe(m):
        return pl.ds(pl.multiple_of(places[m] * quarter, quarter), quarter)

    mix_a = send(mx.at[stripe(1)], mr1.at[0], sent_s.at[MIX], mix_r.at[0], (i, j1))
    mix_b = send(mx.at[stripe(3)], mr1.at[1], sent_s.at[MIX], mix_r.at[1], (i, j1))
    mix_c = send(ms, mr2, sent_s.at[MIX], mix_r.at[2], (i, j2))

    def retention():
        entering = enter[...]
        entering = jnp.where(
            second, spread_rows(tot_in[0]) * entering + st_in[0].astype(F32), entering
        ).astype(BF)
        for h in range(heads):
            c = slice(h * dim, (h + 1) * dim)
            queries = (q_ref[:, c].astype(F32) * jnp.exp(cum[h])).astype(BF)
            kept = inner[:, c] + dot(queries, entering[h * dim : (h + 1) * dim, :])
            unit = kept * lax.rsqrt(jnp.mean(kept * kept, axis=-1, keepdims=True) + epsilon)
            ho[:, c] = (unit * gain_ref[h : h + 1, :] * jax.nn.silu(g_ref[:, c].astype(F32))).astype(BF)
        mx[...] = dot(ho[...], ow[...]).astype(BF)
        mix_b.start()
        mix_a.start()

    def mix_cross():
        mix_b.wait_recv()
        ms[...] = (mx[stripe(2), :].astype(F32) + mr1[1].astype(F32)).astype(BF)

    red, red_y = [], []
    for g in range(CHUNKS):
        r = chunk(g)
        red.append((
            send(part.at[1, r], near.at[0, r], sent_s.at[HALVES], red_r.at[g, 0], (i, j1)),
            send(part.at[3, r], near.at[1, r], sent_s.at[HALVES], red_r.at[g, 1], (i, j1)),
        ))
        for k, p in enumerate(of(g)):
            at = 3 * (g // 2) + (1 + k if across(g) else 0)
            red_y.append(send(half.at[bit(p)], far.at[bit(p)], sent_s.at[SUMS], redy_r.at[at], (i, j2)))

    def summed(p):
        g = p * CHUNKS // PIECES
        if across(g):
            red_y[p].wait_recv()
        elif p == of(g)[0]:
            send(count(step), count(step), sent_s.at[SUMS], redy_r.at[3 * (g // 2)], (i, j2)).wait_recv()

    def gate_up(g, ms, sums=(0.0, 0.0)):
        gate, up = sums
        for m in ms:
            gate = gate + dot(x[m, chunk(g), :], wg[block(m), :])
            up = up + dot(x[m, chunk(g), :], wu[block(m), :])
        return gate, up

    def down(g, sums):
        hidden = (jax.nn.silu(sums[0]) * sums[1]).astype(BF)
        for m in (3, 1, 2, 0):
            part[m, chunk(g), :] = dot(hidden, wd[:, block(m)]).astype(BF)
            if m == 3:
                red[g][1].start()
            if m == 1:
                red[g][0].start()

    def cross(g):
        red[g][1].wait_recv()
        for p in of(g):
            r = bit(p)
            half[r, :] = (part[2, r, :].astype(F32) + near[1, r, :].astype(F32)).astype(BF)
            red_y[p].start()

    groups = [members(0) + members(1), members(4) + members(5), members(2) + members(3), members(6), members(7)]
    ret = [None] * n
    for k, ds in enumerate(groups):
        for d in ds:
            if d:
                ret[d] = send(
                    done.at[slots(d)], back.at[slots(d)], sent_s.at[HOME], ret_r.at[k], (partner(d), j)
                )

    def home(g, which=None):
        if not which:
            red[g][0].wait_recv()
        for p in of(g) if which is None else [of(g)[which]]:
            r = bit(p)
            summed(p)
            done[r, :] = (
                part[0, r, :].astype(F32) + near[0, r, :].astype(F32) + far[r, :].astype(F32)
            ).astype(BF)
            for d in members(p):
                if d:
                    ret[d].start()
                else:
                    back[0:cap, :] = done[0:cap, :]

    forward(1, 0)
    forward(0)
    for c in weight_loads:
        c.wait()
    sums = gate_up(0, (0, 2))
    forward(1, 1)
    arrive(0)
    down(0, gate_up(0, (1, 3), sums))
    sums = gate_up(1, (0,))
    cross(0)
    pair()
    arrive(1)
    sums = gate_up(1, (1,), sums)
    comb = sum(jnp.where(slot == target[t], rw_ref[t : t + 1, :], 0.0) for t in range(top)).T
    hi = comb.astype(BF)
    hi_ref[...] = hi
    lo_ref[...] = (comb - hi.astype(F32)).astype(BF)
    relay(1)
    forward(2)
    sums = gate_up(1, (2,), sums)
    forward(3, 0)
    arrive(1, 1)
    down(1, gate_up(1, (3,), sums))
    forward(3, 1)
    sums = gate_up(2, (0, 2))
    cross(1)
    for r in range(1, rounds - 1):
        absorb(r)
    arrive(2)
    sums = gate_up(2, (1, 3), sums)
    relay(3, 0)
    down(2, sums)
    arrive(3)
    sums = gate_up(3, (0,))
    relay(3, 1)
    sums = gate_up(3, (1,), sums)
    cross(2)
    sums = gate_up(3, (2,), sums)
    home(0)
    arrive(3, 1)
    sums = gate_up(3, (3,), sums)
    home(1, 0)
    down(3, sums)
    home(1, 1)
    cross(3)
    absorb(rounds - 1)
    retention()
    home(2)
    mix_cross()
    mix_c.start()
    home(3, 0)
    home(3, 1)

    def gather(k):
        ds = groups[k]
        r = (len(ds) - (0 in ds)) * cap
        send(count(r), count(r), sent_s.at[HOME], ret_r.at[k], (i, j1)).wait_recv()
        c = slice(position(ds[0]) * cap, position(ds[-1]) * cap + cap)
        return dot(hi_ref[:, c], back[c, :]) + dot(lo_ref[:, c], back[c, :])

    blend = gather(0) + gather(1) + gather(2)
    mix_a.wait_recv()
    mix_c.wait_recv()
    mixer_ref[...] = (
        mx[stripe(0), :].astype(F32) + mr1[0].astype(F32) + mr2[...].astype(F32)
    ).astype(BF)
    blend = blend + gather(3)
    expert_ref[...] = (blend + gather(4)).astype(BF)
    for kind, ref in (
        (DISPATCH, count((n - 1) * cap)), (BOTH, count((n // 2 - 1) * cap)), (ACROSS, count(rows // 2)),
        (CORE, x.at[pl.ds(0, 2)]), (HALVES, x.at[pl.ds(0, 2)]), (SUMS, count(rows)),
        (MIX, mx.at[pl.ds(0, 3 * quarter)]), (HOME, count((n - 1) * cap)),
    ):
        send(ref, ref, sent_s.at[kind], ret_r.at[0], (i, j1)).wait_send()
    st_c[0].wait_send()
    tot_c[0].wait_send()
    for r in range(1, rounds):
        @pl.when(i + (1 << r) < n)
        def _():
            st_c[r].wait_send()
            tot_c[r].wait_send()


def store_kernel(mixer, blended, mixer_out, blended_out, sem):
    copies = [
        pltpu.make_async_copy(mixer, mixer_out, sem.at[0]),
        pltpu.make_async_copy(blended, blended_out, sem.at[1]),
    ]
    for c in copies:
        c.start()
    for c in copies:
        c.wait()


def per_device(
    queries, key_rows, value_rows, out_gate, log_decay, head_gain, out_weight,
    moe_input, moe_gain, expert_gate, expert_up, expert_down, route_ids, route_weights,
):
    n, shares = lax.axis_size("ep"), lax.axis_size("tp")
    tokens, top = route_ids.shape
    pairs = tokens * top
    cap = -(-2 * pairs // n // 16) * 16
    full = moe_input.shape[1]
    width = full // shares
    length, heads = log_decay.shape
    dim = head_gain.shape[1]
    hidden = expert_gate.shape[2]

    rows = n * cap
    rounds = n.bit_length() - 1
    quarter = length // shares
    vmem = pl.BlockSpec(memory_space=pltpu.VMEM)
    hbm = pl.BlockSpec(memory_space=pltpu.HBM)
    dma = pltpu.SemaphoreType.DMA
    args = (
        moe_input, route_ids.T, moe_gain.reshape(1, full), log_decay.T, route_weights.T, head_gain,
        key_rows, value_rows, queries, out_gate, out_weight, expert_gate[0], expert_up[0], expert_down[0],
    )
    args = [pltpu.with_memory_space_constraint(a, pltpu.HBM) for a in args]
    mixer, blended = pl.pallas_call(
        functools.partial(layer_kernel, n, cap, heads),
        out_shape=(
            pltpu.VMEM((quarter, full), BF),
            pltpu.VMEM((tokens, width), BF),
        ),
        in_specs=[hbm] * len(args),
        out_specs=(vmem, vmem),
        scratch_shapes=[pltpu.VMEM(a.shape, a.dtype) for a in args[:6]] + [
            pltpu.VMEM((4, length, heads * dim), BF),
            pltpu.VMEM(out_weight.shape, BF),
            pltpu.VMEM((full, hidden), BF),
            pltpu.VMEM((full, hidden), BF),
            pltpu.VMEM((hidden, full), BF),
            pltpu.VMEM((4, rows, width), BF),
            pltpu.VMEM((4, rows, width), BF),
            pltpu.VMEM((2, rows, width), BF),
            pltpu.VMEM((rows, width), BF),
            pltpu.VMEM((rows, width), BF),
            pltpu.VMEM((rows, width), BF),
            pltpu.VMEM((rows, width), BF),
            pltpu.VMEM((rounds, heads * dim, dim), BF),
            pltpu.VMEM((rounds, heads * dim, dim), BF),
            pltpu.VMEM((rounds, 8, dim), F32),
            pltpu.VMEM((rounds, 8, dim), F32),
            pltpu.VMEM((heads * dim, dim), F32),
            pltpu.VMEM((heads * dim, dim), F32),
            pltpu.VMEM((length, heads * dim), F32),
            pltpu.VMEM((length, heads * dim), BF),
            pltpu.VMEM((length, full), BF),
            pltpu.VMEM((2, quarter, full), BF),
            pltpu.VMEM((quarter, full), BF),
            pltpu.VMEM((quarter, full), BF),
            dma((11,)), dma((8,)), dma((n - 1,)),
            dma((rounds,)), dma((rounds,)), dma((rounds,)), dma((rounds,)),
            dma((PIECES // 2,)), dma((6,)), dma((CHUNKS, 2)), dma((6,)), dma((3,)), dma((5,)),
            pltpu.VMEM((rows, width), BF),
            pltpu.VMEM((rows, width), BF),
            pltpu.VMEM((tokens, rows), BF),
            pltpu.VMEM((tokens, rows), BF),
        ],
        compiler_params=pltpu.CompilerParams(
            collective_id=0, has_side_effects=True, vmem_limit_bytes=56 * 1024 * 1024
        ),
    )(*args)
    return pl.pallas_call(
        store_kernel,
        out_shape=(
            jax.ShapeDtypeStruct(mixer.shape, BF),
            jax.ShapeDtypeStruct(blended.shape, BF),
        ),
        in_specs=[vmem, vmem],
        out_specs=(hbm, hbm),
        scratch_shapes=[dma((2,))],
        compiler_params=pltpu.CompilerParams(vmem_limit_bytes=4 * 1024 * 1024),
    )(mixer, blended)


def solution(mesh):
    in_specs = (
        P("ep", "tp"),
        P("ep", "tp"),
        P("ep", "tp"),
        P("ep", "tp"),
        P("ep", "tp"),
        P("tp", None),
        P("tp", None),
        P("ep", None),
        P(),
        P("ep", None, "tp"),
        P("ep", None, "tp"),
        P("ep", "tp", None),
        P("ep", None),
        P("ep", None),
    )
    out_specs = (P(("ep", "tp"), None), P("ep", "tp"))
    return jax.shard_map(
        per_device, mesh=mesh, in_specs=in_specs, out_specs=out_specs, check_vma=False
    )
```

```python
import functools

import jax
import jax.numpy as jnp
from jax import lax
from jax.experimental import pallas as pl
from jax.experimental.pallas import tpu as pltpu
from jax.sharding import PartitionSpec as P

epsilon = 1e-06
PIECES = 8
GROUPS = ((0,), (2, 3), (4, 5), (6, 7), (1,))
ACROSS_GROUPS = (1, 3)
BF = jnp.bfloat16
F32 = jnp.float32


def dot(a, b, dims=(((1,), (0,)), ((), ()))):
    return lax.dot_general(a, b, dims, preferred_element_type=F32)


def layer_kernel(
    n, cap, heads,
    tok_hbm, ids_hbm, norm_hbm, ld_hbm, rw_hbm, gain_hbm, k_hbm, v_hbm, q_hbm, g_hbm,
    ow_hbm, wg_hbm, wu_hbm, wd_hbm,
    mixer_ref, expert_ref,
    tok_ref, ids_ref, norm_ref, ld_ref, rw_ref, gain_ref, kvqg,
    ow, wg, wu, wd, x, part, near, half, far, done, back,
    st, st_in, tot, tot_in, window, enter, inner, ho, mx, mr1, ms, mr2,
    w_sem, sent_s, disp_r, st_s, st_r, tot_s, tot_r, y_r, c_r, red_r, redy_r, mix_r, ret_r,
    piece_ref, both_ref, hi_ref, lo_ref,
):
    i, j = lax.axis_index("ep"), lax.axis_index("tp")
    j1 = j + 1 - 2 * lax.rem(j, 2)
    j2 = lax.rem(j + 2, 4)
    j3 = lax.rem(j1 + 2, 4)
    places = (j, j1, j2, j3)
    rows = n * cap
    small = rows // PIECES
    width = x.shape[2]
    dim = gain_ref.shape[1]
    k_ref, v_ref, q_ref, g_ref = [kvqg.at[m] for m in range(4)]
    length = kvqg.shape[1]
    quarter = length // 4
    rounds = n.bit_length() - 1

    def partner(d):
        r = i
        for b in range(rounds):
            if (d >> b) & 1:
                r = r + (1 << b) * (1 - 2 * lax.rem(lax.div(i, 1 << b), 2))
        return r

    def position(d):
        return (((d >> 1) & 1) * 2 + d // (n // 2)) * (n // 4) + ((d % (n // 2)) >> 2) * 2 + (d & 1)

    offsets = sorted(range(n), key=position)

    def members(p):
        return [d for d in offsets[p * n // PIECES : (p + 1) * n // PIECES]]

    def slots(d):
        return pl.ds(position(d) * cap, cap)

    def chunk(g):
        return pl.ds(GROUPS[g][0] * small, len(GROUPS[g]) * small)

    def amount(g):
        return len(GROUPS[g]) * small

    def bit(p):
        return pl.ds(p * small, small)

    def of(g):
        return GROUPS[g]

    def across(g):
        return g in ACROSS_GROUPS

    def index(g, which):
        return sum(2 if across(e) else 1 for e in range(g)) + (which if across(g) else 0)

    def send(src, dst, ss, rs, dev):
        return pltpu.make_async_remote_copy(
            src_ref=src, dst_ref=dst, send_sem=ss, recv_sem=rs, device_id=dev,
            device_id_type=pl.DeviceIdType.MESH,
        )

    DISPATCH, BOTH, ACROSS, CORE, HALVES, SUMS, MIX, HOME = range(8)
    small_loads = [
        pltpu.make_async_copy(a, b, w_sem.at[m])
        for m, (a, b) in enumerate((
            (tok_hbm, tok_ref), (ids_hbm, ids_ref), (norm_hbm, norm_ref), (ld_hbm, ld_ref),
            (rw_hbm, rw_ref), (gain_hbm, gain_ref),
        ))
    ]
    head_loads = [
        pltpu.make_async_copy(a, kvqg.at[m], w_sem.at[6]) for m, a in enumerate((k_hbm, v_hbm, q_hbm, g_hbm))
    ]
    weight_loads = [
        pltpu.make_async_copy(a, b, w_sem.at[7 + m])
        for m, (a, b) in enumerate(((ow_hbm, ow), (wg_hbm, wg), (wu_hbm, wu), (wd_hbm, wd)))
    ]
    for c in small_loads + head_loads + weight_loads:
        c.start()
    barrier = pltpu.get_barrier_semaphore()
    for d in range(1, n):
        pl.semaphore_signal(barrier, inc=1, device_id=(partner(d), j), device_id_type=pl.DeviceIdType.MESH)
    for peer in (j1, j2):
        pl.semaphore_signal(barrier, inc=1, device_id=(i, peer), device_id_type=pl.DeviceIdType.MESH)

    def block(m):
        return pl.ds(pl.multiple_of(places[m] * width, width), width)

    top, tokens = ids_ref.shape
    lanes = -(-n // 16) * 16
    small_loads[1].wait()
    expert = lax.broadcasted_iota(jnp.int32, (lanes, tokens), 0)
    named = [ids_ref[t : t + 1, :] == expert for t in range(top)]
    strict = lax.broadcasted_iota(jnp.int32, (tokens, tokens), 0) < lax.broadcasted_iota(
        jnp.int32, (tokens, tokens), 1
    )
    held = sum(jnp.where(m, 1.0, 0.0) for m in named)
    before = dot(held.astype(BF), jnp.where(strict, 1.0, 0.0).astype(BF))
    slot = lax.broadcasted_iota(jnp.int32, (rows, tokens), 0)
    target = []
    for t in range(top):
        rank = jnp.sum(jnp.where(named[t], before, 0.0), axis=0, keepdims=True).astype(jnp.int32)
        d = jnp.bitwise_xor(ids_ref[t : t + 1, :], i)
        over = jnp.where(d >= n // 2, 1, 0)
        kept = d - over * (n // 2)
        place = ((d >> 1) & 1) * 2 + over
        place = place * (n // 4) + (kept >> 2) * 2 + (d & 1)
        target.append(place * cap + rank)
    pick = sum(jnp.where(slot == target[t], 1.0, 0.0) for t in range(top)).astype(BF)
    small_loads[0].wait()
    small_loads[2].wait()
    rows_f = tok_ref[...].astype(F32)
    scale = lax.rsqrt(jnp.mean(rows_f * rows_f, axis=-1, keepdims=True) + epsilon)

    def normed(m):
        return (tok_ref[:, block(m)].astype(F32) * scale * norm_ref[:, block(m)]).astype(BF)

    piece = dot(pick, normed(0)).astype(BF)
    piece_ref[...] = piece
    x[0, 0:cap, :] = piece[0:cap]
    pl.semaphore_wait(barrier, n + 1)

    def count(r):
        return x.at[0, pl.ds(0, r)]

    disp, disp2 = [None] * n, [None] * n
    for d in range(1, n):
        to = (partner(d), j)
        disp[d] = send(piece_ref.at[slots(d)], x.at[0, slots(d)], sent_s.at[DISPATCH], disp_r.at[d - 1], to)
        if d < n // 2:
            disp2[d] = send(both_ref.at[slots(d)], x.at[2, slots(d)], sent_s.at[BOTH], disp_r.at[d - 1], to)

    def dispatch(g, which=None):
        for p in of(g) if which is None else [of(g)[which]]:
            for d in members(p):
                if d:
                    disp[d].start()
                    if not across(g):
                        disp2[d].start()

    def dispatched(d):
        rows_in = cap if d >= n // 2 else 2 * cap
        send(count(rows_in), count(rows_in), sent_s.at[DISPATCH], disp_r.at[d - 1], (partner(d), j)).wait_recv()

    dispatch(1, 0)
    both = normed(2)
    for a in (0, rows // 2):
        r = slice(a, a + rows // 4)
        both_ref[r, :] = dot(pick[r], both).astype(BF)
    x[2, 0:cap, :] = both_ref[0:cap, :]
    dispatch(0)
    dispatch(4)
    dispatch(1, 1)

    pieces_across = [p for g in ACROSS_GROUPS for p in of(g)]
    y_c, c0_c, c2_c = [None] * PIECES, [None] * PIECES, [None] * PIECES
    for g in range(len(GROUPS)):
        for p in of(g):
            r = bit(p)
            if across(g):
                y_c[p] = send(
                    x.at[0, r], x.at[2, r], sent_s.at[ACROSS], y_r.at[pieces_across.index(p)], (i, j2)
                )
            c0_c[p] = send(x.at[0, r], x.at[1, r], sent_s.at[CORE], c_r.at[index(g, 0)], (i, j1))
            c2_c[p] = send(x.at[2, r], x.at[3, r], sent_s.at[CORE], c_r.at[index(g, 1)], (i, j1))

    def arrive(g, which=0):
        rows_in = amount(g) if across(g) else 2 * amount(g)
        send(count(rows_in), count(rows_in), sent_s.at[CORE], c_r.at[index(g, which)], (i, j1)).wait_recv()

    def forward(g, which=None):
        for p in of(g) if which is None else [of(g)[which]]:
            for d in members(p):
                if d:
                    dispatched(d)
            if across(g):
                y_c[p].start()
            else:
                c2_c[p].start()
            c0_c[p].start()

    def relay(g, which=None):
        for p in of(g) if which is None else [of(g)[which]]:
            y_c[p].wait_recv()
            c2_c[p].start()

    causal = lax.broadcasted_iota(jnp.int32, (length, length), 0) >= lax.broadcasted_iota(
        jnp.int32, (length, length), 1
    )
    upper = jnp.where(
        lax.broadcasted_iota(jnp.int32, (length, length), 0)
        <= lax.broadcasted_iota(jnp.int32, (length, length), 1), 1.0, 0.0
    )
    for c in small_loads[3:]:
        c.wait()
    pltpu.make_async_copy(kvqg, kvqg, w_sem.at[6]).wait()
    level = lax.dot_general(
        ld_ref[...], upper, (((1,), (0,)), ((), ())),
        precision=lax.Precision.HIGHEST, preferred_element_type=F32,
    )
    cum = [jnp.broadcast_to(level[h : h + 1, :], (dim, length)).T for h in range(heads)]
    tot[0] = jnp.zeros(tot.shape[1:], F32)
    for h in range(heads):
        c = slice(h * dim, (h + 1) * dim)
        total = cum[h][length - 1 : length, :]
        keys = k_ref[:, c].astype(F32) * jnp.exp(total - cum[h])
        window[c, :] = dot(keys.T.astype(BF), v_ref[:, c])
        tot[0, h : h + 1, :] = total
    st[0] = window[...].astype(BF)
    enter[...] = jnp.zeros_like(enter)
    st_c, tot_c = [], []
    for r in range(rounds):
        later = (lax.rem(i + (1 << r), n) if r else partner(1), j)
        st_c.append(send(st.at[r], st_in.at[r], st_s.at[r], st_r.at[r], later))
        tot_c.append(send(tot.at[r], tot_in.at[r], tot_s.at[r], tot_r.at[r], later))

    second = lax.rem(i, 2) == 1

    def pass_on(r):
        @pl.when(i + (1 << r) < n)
        def _():
            st_c[r].start()
            tot_c[r].start()

    span = [jnp.zeros(tot.shape[1:], F32)]

    def spread_rows(totals):
        return jnp.concatenate(
            [jnp.broadcast_to(jnp.exp(totals[h : h + 1, :]), (dim, dim)) for h in range(heads)], axis=0
        )

    def pair():
        st_c[0].wait_recv()
        tot_c[0].wait_recv()
        own, arrived = window[...], st_in[0].astype(F32)
        late = spread_rows(jnp.where(second, tot[0], tot_in[0]))
        window[...] = late * jnp.where(second, arrived, own) + jnp.where(second, own, arrived)
        st[1] = window[...].astype(BF)
        tot[1] = tot[0] + tot_in[0]
        pass_on(1)

    def absorb(r):
        @pl.when(i >= 1 << r)
        def _():
            st_c[r].wait_recv()
            tot_c[r].wait_recv()

        @pl.when(i < 1 << r)
        def _():
            st_in[r] = jnp.zeros(st_in.shape[1:], BF)
            tot_in[r] = jnp.zeros(tot_in.shape[1:], F32)

        arrived = st_in[r].astype(F32)
        enter[...] = spread_rows(span[0]) * arrived + enter[...]
        span[0] = span[0] + tot_in[r]
        if r + 1 < rounds:
            window[...] = spread_rows(tot[r]) * arrived + window[...]
            st[r + 1] = window[...].astype(BF)
            tot[r + 1] = tot[r] + tot_in[r]
            pass_on(r + 1)

    forward(0)
    st_c[0].start()
    tot_c[0].start()
    dispatch(2)
    dispatch(3)

    for h in range(heads):
        c = slice(h * dim, (h + 1) * dim)
        scores = dot(q_ref[:, c], k_ref[:, c], (((1,), (1,)), ((), ()))) * dim ** (-0.5)
        spread = jnp.where(causal, cum[h][:, 0:1] - level[h : h + 1, :], -jnp.inf)
        inner[:, c] = dot((scores * jnp.exp(spread)).astype(BF), v_ref[:, c])

    def stripe(m):
        return pl.ds(pl.multiple_of(places[m] * quarter, quarter), quarter)

    mix_a = send(mx.at[stripe(1)], mr1.at[0], sent_s.at[MIX], mix_r.at[0], (i, j1))
    mix_b = send(mx.at[stripe(3)], mr1.at[1], sent_s.at[MIX], mix_r.at[1], (i, j1))
    mix_c = send(ms, mr2, sent_s.at[MIX], mix_r.at[2], (i, j2))

    def retention():
        entering = enter[...]
        entering = jnp.where(
            second, spread_rows(tot_in[0]) * entering + st_in[0].astype(F32), entering
        ).astype(BF)
        for h in range(heads):
            c = slice(h * dim, (h + 1) * dim)
            queries = (q_ref[:, c].astype(F32) * jnp.exp(cum[h])).astype(BF)
            kept = inner[:, c] + dot(queries, entering[h * dim : (h + 1) * dim, :])
            unit = kept * lax.rsqrt(jnp.mean(kept * kept, axis=-1, keepdims=True) + epsilon)
            ho[:, c] = (unit * gain_ref[h : h + 1, :] * jax.nn.silu(g_ref[:, c].astype(F32))).astype(BF)
        mx[...] = dot(ho[...], ow[...]).astype(BF)
        mix_b.start()
        mix_a.start()

    def mix_cross():
        mix_b.wait_recv()
        ms[...] = (mx[stripe(2), :].astype(F32) + mr1[1].astype(F32)).astype(BF)

    red, red_y = [], [None] * PIECES
    for g in range(len(GROUPS)):
        r = chunk(g)
        red.append((
            send(part.at[1, r], near.at[0, r], sent_s.at[HALVES], red_r.at[g, 0], (i, j1)),
            send(part.at[3, r], near.at[1, r], sent_s.at[HALVES], red_r.at[g, 1], (i, j1)),
        ))
        for k, p in enumerate(of(g)):
            red_y[p] = send(half.at[bit(p)], far.at[bit(p)], sent_s.at[SUMS], redy_r.at[index(g, k)], (i, j2))

    def summed(g, k):
        if across(g):
            red_y[of(g)[k]].wait_recv()
        elif k == 0:
            r = amount(g)
            send(count(r), count(r), sent_s.at[SUMS], redy_r.at[index(g, 0)], (i, j2)).wait_recv()

    def gate_up(g, ms, sums=(0.0, 0.0)):
        gate, up = sums
        for m in ms:
            gate = gate + dot(x[m, chunk(g), :], wg[block(m), :])
            up = up + dot(x[m, chunk(g), :], wu[block(m), :])
        return gate, up

    def down(g, sums):
        hidden = (jax.nn.silu(sums[0]) * sums[1]).astype(BF)
        for m in (3, 1, 2, 0):
            part[m, chunk(g), :] = dot(hidden, wd[:, block(m)]).astype(BF)
            if m == 3:
                red[g][1].start()
            if m == 1:
                red[g][0].start()

    def cross(g):
        red[g][1].wait_recv()
        for p in of(g):
            r = bit(p)
            half[r, :] = (part[2, r, :].astype(F32) + near[1, r, :].astype(F32)).astype(BF)
            red_y[p].start()

    groups = [members(0) + members(1), members(4) + members(5), members(2) + members(3), members(6), members(7)]
    ret = [None] * n
    for k, ds in enumerate(groups):
        for d in ds:
            if d:
                ret[d] = send(
                    done.at[slots(d)], back.at[slots(d)], sent_s.at[HOME], ret_r.at[k], (partner(d), j)
                )

    def home(g, which=None):
        if not which:
            red[g][0].wait_recv()
        for k in range(len(of(g))) if which is None else [which]:
            p = of(g)[k]
            r = bit(p)
            summed(g, k)
            done[r, :] = (
                part[0, r, :].astype(F32) + near[0, r, :].astype(F32) + far[r, :].astype(F32)
            ).astype(BF)
            for d in members(p):
                if d:
                    ret[d].start()
                else:
                    back[0:cap, :] = done[0:cap, :]

    for c in weight_loads:
        c.wait()
    arrive(0)
    down(0, gate_up(0, (0, 2, 1, 3)))
    forward(1, 0)
    forward(4)
    sums = gate_up(4, (0, 2))
    forward(1, 1)
    cross(0)
    arrive(4)
    down(4, gate_up(4, (1, 3), sums))
    sums = gate_up(1, (0,))
    cross(4)
    pair()
    arrive(1)
    sums = gate_up(1, (1,), sums)
    comb = sum(jnp.where(slot == target[t], rw_ref[t : t + 1, :], 0.0) for t in range(top)).T
    hi = comb.astype(BF)
    hi_ref[...] = hi
    lo_ref[...] = (comb - hi.astype(F32)).astype(BF)
    relay(1)
    sums = gate_up(1, (2,), sums)
    forward(3, 0)
    arrive(1, 1)
    down(1, gate_up(1, (3,), sums))
    forward(2)
    forward(3, 1)
    sums = gate_up(2, (0, 2))
    cross(1)
    arrive(2)
    sums = gate_up(2, (1, 3), sums)
    for r in range(1, rounds - 1):
        absorb(r)
    relay(3, 0)
    down(2, sums)
    arrive(3)
    sums = gate_up(3, (0,))
    relay(3, 1)
    sums = gate_up(3, (1,), sums)
    cross(2)
    sums = gate_up(3, (2,), sums)
    home(1, 0)
    arrive(3, 1)
    down(3, gate_up(3, (3,), sums))
    home(1, 1)
    home(0)
    cross(3)
    home(4)
    absorb(rounds - 1)
    retention()
    home(2)
    mix_cross()
    mix_c.start()
    home(3, 0)
    home(3, 1)

    def gather(k):
        ds = groups[k]
        r = (len(ds) - (0 in ds)) * cap
        send(count(r), count(r), sent_s.at[HOME], ret_r.at[k], (i, j1)).wait_recv()
        c = slice(position(ds[0]) * cap, position(ds[-1]) * cap + cap)
        return dot(hi_ref[:, c], back[c, :]) + dot(lo_ref[:, c], back[c, :])

    blend = gather(0) + gather(1) + gather(2)
    mix_a.wait_recv()
    mix_c.wait_recv()
    mixer_ref[...] = (
        mx[stripe(0), :].astype(F32) + mr1[0].astype(F32) + mr2[...].astype(F32)
    ).astype(BF)
    blend = blend + gather(3)
    expert_ref[...] = (blend + gather(4)).astype(BF)
    for kind, ref in (
        (DISPATCH, count((n - 1) * cap)), (BOTH, count((n // 2 - 1) * cap)), (ACROSS, count(rows // 2)),
        (CORE, x.at[pl.ds(0, 2)]), (HALVES, x.at[pl.ds(0, 2)]), (SUMS, count(rows)),
        (MIX, mx.at[pl.ds(0, 3 * quarter)]), (HOME, count((n - 1) * cap)),
    ):
        send(ref, ref, sent_s.at[kind], ret_r.at[0], (i, j1)).wait_send()
    st_c[0].wait_send()
    tot_c[0].wait_send()
    for r in range(1, rounds):
        @pl.when(i + (1 << r) < n)
        def _():
            st_c[r].wait_send()
            tot_c[r].wait_send()


def store_kernel(mixer, blended, mixer_out, blended_out, sem):
    copies = [
        pltpu.make_async_copy(mixer, mixer_out, sem.at[0]),
        pltpu.make_async_copy(blended, blended_out, sem.at[1]),
    ]
    for c in copies:
        c.start()
    for c in copies:
        c.wait()


def per_device(
    queries, key_rows, value_rows, out_gate, log_decay, head_gain, out_weight,
    moe_input, moe_gain, expert_gate, expert_up, expert_down, route_ids, route_weights,
):
    n, shares = lax.axis_size("ep"), lax.axis_size("tp")
    tokens, top = route_ids.shape
    pairs = tokens * top
    cap = -(-2 * pairs // n // 16) * 16
    full = moe_input.shape[1]
    width = full // shares
    length, heads = log_decay.shape
    dim = head_gain.shape[1]
    hidden = expert_gate.shape[2]

    rows = n * cap
    rounds = n.bit_length() - 1
    quarter = length // shares
    vmem = pl.BlockSpec(memory_space=pltpu.VMEM)
    hbm = pl.BlockSpec(memory_space=pltpu.HBM)
    dma = pltpu.SemaphoreType.DMA
    args = (
        moe_input, route_ids.T, moe_gain.reshape(1, full), log_decay.T, route_weights.T, head_gain,
        key_rows, value_rows, queries, out_gate, out_weight, expert_gate[0], expert_up[0], expert_down[0],
    )
    args = [pltpu.with_memory_space_constraint(a, pltpu.HBM) for a in args]
    mixer, blended = pl.pallas_call(
        functools.partial(layer_kernel, n, cap, heads),
        out_shape=(
            pltpu.VMEM((quarter, full), BF),
            pltpu.VMEM((tokens, width), BF),
        ),
        in_specs=[hbm] * len(args),
        out_specs=(vmem, vmem),
        scratch_shapes=[pltpu.VMEM(a.shape, a.dtype) for a in args[:6]] + [
            pltpu.VMEM((4, length, heads * dim), BF),
            pltpu.VMEM(out_weight.shape, BF),
            pltpu.VMEM((full, hidden), BF),
            pltpu.VMEM((full, hidden), BF),
            pltpu.VMEM((hidden, full), BF),
            pltpu.VMEM((4, rows, width), BF),
            pltpu.VMEM((4, rows, width), BF),
            pltpu.VMEM((2, rows, width), BF),
            pltpu.VMEM((rows, width), BF),
            pltpu.VMEM((rows, width), BF),
            pltpu.VMEM((rows, width), BF),
            pltpu.VMEM((rows, width), BF),
            pltpu.VMEM((rounds, heads * dim, dim), BF),
            pltpu.VMEM((rounds, heads * dim, dim), BF),
            pltpu.VMEM((rounds, 8, dim), F32),
            pltpu.VMEM((rounds, 8, dim), F32),
            pltpu.VMEM((heads * dim, dim), F32),
            pltpu.VMEM((heads * dim, dim), F32),
            pltpu.VMEM((length, heads * dim), F32),
            pltpu.VMEM((length, heads * dim), BF),
            pltpu.VMEM((length, full), BF),
            pltpu.VMEM((2, quarter, full), BF),
            pltpu.VMEM((quarter, full), BF),
            pltpu.VMEM((quarter, full), BF),
            dma((11,)), dma((8,)), dma((n - 1,)),
            dma((rounds,)), dma((rounds,)), dma((rounds,)), dma((rounds,)),
            dma((PIECES // 2,)), dma((7,)), dma((len(GROUPS), 2)), dma((7,)), dma((3,)), dma((5,)),
            pltpu.VMEM((rows, width), BF),
            pltpu.VMEM((rows, width), BF),
            pltpu.VMEM((tokens, rows), BF),
            pltpu.VMEM((tokens, rows), BF),
        ],
        compiler_params=pltpu.CompilerParams(
            collective_id=0, has_side_effects=True, vmem_limit_bytes=56 * 1024 * 1024
        ),
    )(*args)
    return pl.pallas_call(
        store_kernel,
        out_shape=(
            jax.ShapeDtypeStruct(mixer.shape, BF),
            jax.ShapeDtypeStruct(blended.shape, BF),
        ),
        in_specs=[vmem, vmem],
        out_specs=(hbm, hbm),
        scratch_shapes=[dma((2,))],
        compiler_params=pltpu.CompilerParams(vmem_limit_bytes=4 * 1024 * 1024),
    )(mixer, blended)


def solution(mesh):
    in_specs = (
        P("ep", "tp"),
        P("ep", "tp"),
        P("ep", "tp"),
        P("ep", "tp"),
        P("ep", "tp"),
        P("tp", None),
        P("tp", None),
        P("ep", None),
        P(),
        P("ep", None, "tp"),
        P("ep", None, "tp"),
        P("ep", "tp", None),
        P("ep", None),
        P("ep", None),
    )
    out_specs = (P(("ep", "tp"), None), P("ep", "tp"))
    return jax.shard_map(
        per_device, mesh=mesh, in_specs=in_specs, out_specs=out_specs, check_vma=False
    )
```

```python
import functools

import jax
import jax.numpy as jnp
from jax import lax
from jax.experimental import pallas as pl
from jax.experimental.pallas import tpu as pltpu
from jax.sharding import PartitionSpec as P

epsilon = 1e-06
PIECES = 8
GROUPS = ((0,), (2, 3), (4, 5), (6, 7), (1,))
ACROSS_GROUPS = (1, 3)
BF = jnp.bfloat16
F32 = jnp.float32


def dot(a, b, dims=(((1,), (0,)), ((), ()))):
    return lax.dot_general(a, b, dims, preferred_element_type=F32)


def layer_kernel(
    n, cap, heads,
    tok_hbm, ids_hbm, norm_hbm, ld_hbm, rw_hbm, gain_hbm, k_hbm, v_hbm, q_hbm, g_hbm,
    ow_hbm, wg_hbm, wu_hbm, wd_hbm,
    mixer_ref, expert_ref,
    tok_ref, ids_ref, norm_ref, ld_ref, rw_ref, gain_ref, kvqg,
    ow, wg, wu, wd, x, part, near, half, far, done, back,
    st, st_in, tot, tot_in, window, enter, inner, ho, mx, mr1, ms, mr2,
    w_sem, sent_s, disp_r, st_s, st_r, tot_s, tot_r, y_r, c_r, red_r, redy_r, mix_r, ret_r,
    piece_ref, both_ref, hi_ref, lo_ref, scaled, opened,
):
    i, j = lax.axis_index("ep"), lax.axis_index("tp")
    j1 = j + 1 - 2 * lax.rem(j, 2)
    j2 = lax.rem(j + 2, 4)
    j3 = lax.rem(j1 + 2, 4)
    places = (j, j1, j2, j3)
    rows = n * cap
    small = rows // PIECES
    width = x.shape[2]
    dim = gain_ref.shape[1]
    k_ref, v_ref, q_ref, g_ref = [kvqg.at[m] for m in range(4)]
    length = kvqg.shape[1]
    quarter = length // 4
    rounds = n.bit_length() - 1

    def partner(d):
        r = i
        for b in range(rounds):
            if (d >> b) & 1:
                r = r + (1 << b) * (1 - 2 * lax.rem(lax.div(i, 1 << b), 2))
        return r

    def position(d):
        return (((d >> 1) & 1) * 2 + d // (n // 2)) * (n // 4) + ((d % (n // 2)) >> 2) * 2 + (d & 1)

    offsets = sorted(range(n), key=position)

    def members(p):
        return [d for d in offsets[p * n // PIECES : (p + 1) * n // PIECES]]

    def slots(d):
        return pl.ds(position(d) * cap, cap)

    def chunk(g):
        return pl.ds(GROUPS[g][0] * small, len(GROUPS[g]) * small)

    def amount(g):
        return len(GROUPS[g]) * small

    def bit(p):
        return pl.ds(p * small, small)

    def of(g):
        return GROUPS[g]

    def across(g):
        return g in ACROSS_GROUPS

    def index(g, which):
        return sum(2 if across(e) else 1 for e in range(g)) + (which if across(g) else 0)

    def send(src, dst, ss, rs, dev):
        return pltpu.make_async_remote_copy(
            src_ref=src, dst_ref=dst, send_sem=ss, recv_sem=rs, device_id=dev,
            device_id_type=pl.DeviceIdType.MESH,
        )

    DISPATCH, BOTH, ACROSS, CORE, HALVES, SUMS, MIX, HOME = range(8)
    small_loads = [
        pltpu.make_async_copy(a, b, w_sem.at[m])
        for m, (a, b) in enumerate((
            (tok_hbm, tok_ref), (ids_hbm, ids_ref), (norm_hbm, norm_ref), (ld_hbm, ld_ref),
            (rw_hbm, rw_ref), (gain_hbm, gain_ref),
        ))
    ]
    head_loads = [
        pltpu.make_async_copy(a, kvqg.at[m], w_sem.at[6]) for m, a in enumerate((k_hbm, v_hbm, q_hbm, g_hbm))
    ]
    weight_loads = [
        pltpu.make_async_copy(a, b, w_sem.at[7 + m])
        for m, (a, b) in enumerate(((ow_hbm, ow), (wg_hbm, wg), (wu_hbm, wu), (wd_hbm, wd)))
    ]
    for c in small_loads + head_loads + weight_loads:
        c.start()
    barrier = pltpu.get_barrier_semaphore()
    for d in range(1, n):
        pl.semaphore_signal(barrier, inc=1, device_id=(partner(d), j), device_id_type=pl.DeviceIdType.MESH)
    for peer in (j1, j2):
        pl.semaphore_signal(barrier, inc=1, device_id=(i, peer), device_id_type=pl.DeviceIdType.MESH)

    def block(m):
        return pl.ds(pl.multiple_of(places[m] * width, width), width)

    top, tokens = ids_ref.shape
    lanes = -(-n // 16) * 16
    small_loads[1].wait()
    expert = lax.broadcasted_iota(jnp.int32, (lanes, tokens), 0)
    named = [ids_ref[t : t + 1, :] == expert for t in range(top)]
    strict = lax.broadcasted_iota(jnp.int32, (tokens, tokens), 0) < lax.broadcasted_iota(
        jnp.int32, (tokens, tokens), 1
    )
    held = sum(jnp.where(m, 1.0, 0.0) for m in named)
    before = dot(held.astype(BF), jnp.where(strict, 1.0, 0.0).astype(BF))
    slot = lax.broadcasted_iota(jnp.int32, (rows, tokens), 0)
    target = []
    for t in range(top):
        rank = jnp.sum(jnp.where(named[t], before, 0.0), axis=0, keepdims=True).astype(jnp.int32)
        d = jnp.bitwise_xor(ids_ref[t : t + 1, :], i)
        over = jnp.where(d >= n // 2, 1, 0)
        kept = d - over * (n // 2)
        place = ((d >> 1) & 1) * 2 + over
        place = place * (n // 4) + (kept >> 2) * 2 + (d & 1)
        target.append(place * cap + rank)
    pick = sum(jnp.where(slot == target[t], 1.0, 0.0) for t in range(top)).astype(BF)
    small_loads[0].wait()
    small_loads[2].wait()
    rows_f = tok_ref[...].astype(F32)
    scale = lax.rsqrt(jnp.mean(rows_f * rows_f, axis=-1, keepdims=True) + epsilon)

    def normed(m):
        return (tok_ref[:, block(m)].astype(F32) * scale * norm_ref[:, block(m)]).astype(BF)

    piece = dot(pick, normed(0)).astype(BF)
    piece_ref[...] = piece
    x[0, 0:cap, :] = piece[0:cap]
    pl.semaphore_wait(barrier, n + 1)

    def count(r):
        return x.at[0, pl.ds(0, r)]

    disp, disp2 = [None] * n, [None] * n
    for d in range(1, n):
        to = (partner(d), j)
        disp[d] = send(piece_ref.at[slots(d)], x.at[0, slots(d)], sent_s.at[DISPATCH], disp_r.at[d - 1], to)
        if d < n // 2:
            disp2[d] = send(both_ref.at[slots(d)], x.at[2, slots(d)], sent_s.at[BOTH], disp_r.at[d - 1], to)

    def dispatch(g, which=None):
        for p in of(g) if which is None else [of(g)[which]]:
            for d in members(p):
                if d:
                    disp[d].start()
                    if not across(g):
                        disp2[d].start()

    def dispatched(d):
        rows_in = cap if d >= n // 2 else 2 * cap
        send(count(rows_in), count(rows_in), sent_s.at[DISPATCH], disp_r.at[d - 1], (partner(d), j)).wait_recv()

    dispatch(1, 0)
    both = normed(2)
    for a in (0, rows // 2):
        r = slice(a, a + rows // 4)
        both_ref[r, :] = dot(pick[r], both).astype(BF)
    x[2, 0:cap, :] = both_ref[0:cap, :]
    dispatch(0)
    dispatch(4)
    dispatch(1, 1)

    pieces_across = [p for g in ACROSS_GROUPS for p in of(g)]
    y_c, c0_c, c2_c = [None] * PIECES, [None] * PIECES, [None] * PIECES
    for g in range(len(GROUPS)):
        for p in of(g):
            r = bit(p)
            if across(g):
                y_c[p] = send(
                    x.at[0, r], x.at[2, r], sent_s.at[ACROSS], y_r.at[pieces_across.index(p)], (i, j2)
                )
            c0_c[p] = send(x.at[0, r], x.at[1, r], sent_s.at[CORE], c_r.at[index(g, 0)], (i, j1))
            c2_c[p] = send(x.at[2, r], x.at[3, r], sent_s.at[CORE], c_r.at[index(g, 1)], (i, j1))

    def arrive(g, which=0):
        rows_in = amount(g) if across(g) else 2 * amount(g)
        send(count(rows_in), count(rows_in), sent_s.at[CORE], c_r.at[index(g, which)], (i, j1)).wait_recv()

    def forward(g, which=None):
        for p in of(g) if which is None else [of(g)[which]]:
            for d in members(p):
                if d:
                    dispatched(d)
            if across(g):
                y_c[p].start()
            else:
                c2_c[p].start()
            c0_c[p].start()

    def relay(g, which=None):
        for p in of(g) if which is None else [of(g)[which]]:
            y_c[p].wait_recv()
            c2_c[p].start()

    causal = lax.broadcasted_iota(jnp.int32, (length, length), 0) >= lax.broadcasted_iota(
        jnp.int32, (length, length), 1
    )
    upper = jnp.where(
        lax.broadcasted_iota(jnp.int32, (length, length), 0)
        <= lax.broadcasted_iota(jnp.int32, (length, length), 1), 1.0, 0.0
    )
    for c in small_loads[3:]:
        c.wait()
    pltpu.make_async_copy(kvqg, kvqg, w_sem.at[6]).wait()
    level = lax.dot_general(
        ld_ref[...], upper, (((1,), (0,)), ((), ())),
        precision=lax.Precision.HIGHEST, preferred_element_type=F32,
    )
    cum = [jnp.broadcast_to(level[h : h + 1, :], (dim, length)).T for h in range(heads)]
    tot[0] = jnp.zeros(tot.shape[1:], F32)
    for h in range(heads):
        c = slice(h * dim, (h + 1) * dim)
        total = cum[h][length - 1 : length, :]
        keys = k_ref[:, c].astype(F32) * jnp.exp(total - cum[h])
        window[c, :] = dot(keys.T.astype(BF), v_ref[:, c])
        tot[0, h : h + 1, :] = total
    st[0] = window[...].astype(BF)
    enter[...] = jnp.zeros_like(enter)
    st_c, tot_c = [], []
    for r in range(rounds):
        later = (lax.rem(i + (1 << r), n) if r else partner(1), j)
        st_c.append(send(st.at[r], st_in.at[r], st_s.at[r], st_r.at[r], later))
        tot_c.append(send(tot.at[r], tot_in.at[r], tot_s.at[r], tot_r.at[r], later))

    second = lax.rem(i, 2) == 1

    def pass_on(r):
        @pl.when(i + (1 << r) < n)
        def _():
            st_c[r].start()
            tot_c[r].start()

    span = [jnp.zeros(tot.shape[1:], F32)]

    def spread_rows(totals):
        return jnp.concatenate(
            [jnp.broadcast_to(jnp.exp(totals[h : h + 1, :]), (dim, dim)) for h in range(heads)], axis=0
        )

    def pair():
        st_c[0].wait_recv()
        tot_c[0].wait_recv()
        own, arrived = window[...], st_in[0].astype(F32)
        late = spread_rows(jnp.where(second, tot[0], tot_in[0]))
        window[...] = late * jnp.where(second, arrived, own) + jnp.where(second, own, arrived)
        st[1] = window[...].astype(BF)
        tot[1] = tot[0] + tot_in[0]
        pass_on(1)

    def absorb(r):
        @pl.when(i >= 1 << r)
        def _():
            st_c[r].wait_recv()
            tot_c[r].wait_recv()

        @pl.when(i < 1 << r)
        def _():
            st_in[r] = jnp.zeros(st_in.shape[1:], BF)
            tot_in[r] = jnp.zeros(tot_in.shape[1:], F32)

        arrived = st_in[r].astype(F32)
        enter[...] = spread_rows(span[0]) * arrived + enter[...]
        span[0] = span[0] + tot_in[r]
        if r + 1 < rounds:
            window[...] = spread_rows(tot[r]) * arrived + window[...]
            st[r + 1] = window[...].astype(BF)
            tot[r + 1] = tot[r] + tot_in[r]
            pass_on(r + 1)

    forward(0)
    st_c[0].start()
    tot_c[0].start()
    dispatch(2)
    dispatch(3)

    for h in range(heads):
        c = slice(h * dim, (h + 1) * dim)
        scores = dot(q_ref[:, c], k_ref[:, c], (((1,), (1,)), ((), ()))) * dim ** (-0.5)
        spread = jnp.where(causal, cum[h][:, 0:1] - level[h : h + 1, :], -jnp.inf)
        inner[:, c] = dot((scores * jnp.exp(spread)).astype(BF), v_ref[:, c])
        scaled[:, c] = (q_ref[:, c].astype(F32) * jnp.exp(cum[h])).astype(BF)
        opened[:, c] = jax.nn.silu(g_ref[:, c].astype(F32))

    def stripe(m):
        return pl.ds(pl.multiple_of(places[m] * quarter, quarter), quarter)

    mix_a = send(mx.at[stripe(1)], mr1.at[0], sent_s.at[MIX], mix_r.at[0], (i, j1))
    mix_b = send(mx.at[stripe(3)], mr1.at[1], sent_s.at[MIX], mix_r.at[1], (i, j1))
    mix_c = send(ms, mr2, sent_s.at[MIX], mix_r.at[2], (i, j2))

    def retention():
        entering = enter[...]
        entering = jnp.where(
            second, spread_rows(tot_in[0]) * entering + st_in[0].astype(F32), entering
        ).astype(BF)
        for h in range(heads):
            c = slice(h * dim, (h + 1) * dim)
            kept = inner[:, c] + dot(scaled[:, c], entering[h * dim : (h + 1) * dim, :])
            unit = kept * lax.rsqrt(jnp.mean(kept * kept, axis=-1, keepdims=True) + epsilon)
            ho[:, c] = (unit * gain_ref[h : h + 1, :] * opened[:, c]).astype(BF)
        mx[...] = dot(ho[...], ow[...]).astype(BF)
        mix_b.start()
        mix_a.start()

    def mix_cross():
        mix_b.wait_recv()
        ms[...] = (mx[stripe(2), :].astype(F32) + mr1[1].astype(F32)).astype(BF)

    red, red_y = [], [None] * PIECES
    for g in range(len(GROUPS)):
        r = chunk(g)
        red.append((
            send(part.at[1, r], near.at[0, r], sent_s.at[HALVES], red_r.at[g, 0], (i, j1)),
            send(part.at[3, r], near.at[1, r], sent_s.at[HALVES], red_r.at[g, 1], (i, j1)),
        ))
        for k, p in enumerate(of(g)):
            red_y[p] = send(half.at[bit(p)], far.at[bit(p)], sent_s.at[SUMS], redy_r.at[index(g, k)], (i, j2))

    def summed(g, k):
        if across(g):
            red_y[of(g)[k]].wait_recv()
        elif k == 0:
            r = amount(g)
            send(count(r), count(r), sent_s.at[SUMS], redy_r.at[index(g, 0)], (i, j2)).wait_recv()

    def gate_up(g, ms, sums=(0.0, 0.0)):
        gate, up = sums
        for m in ms:
            gate = gate + dot(x[m, chunk(g), :], wg[block(m), :])
            up = up + dot(x[m, chunk(g), :], wu[block(m), :])
        return gate, up

    def down(g, sums):
        hidden = (jax.nn.silu(sums[0]) * sums[1]).astype(BF)
        for m in (3, 1, 2, 0):
            part[m, chunk(g), :] = dot(hidden, wd[:, block(m)]).astype(BF)
            if m == 3:
                red[g][1].start()
            if m == 1:
                red[g][0].start()

    def cross(g):
        red[g][1].wait_recv()
        for p in of(g):
            r = bit(p)
            half[r, :] = (part[2, r, :].astype(F32) + near[1, r, :].astype(F32)).astype(BF)
            red_y[p].start()

    groups = [members(0) + members(1), members(4) + members(5), members(2) + members(3), members(6), members(7)]
    ret = [None] * n
    for k, ds in enumerate(groups):
        for d in ds:
            if d:
                ret[d] = send(
                    done.at[slots(d)], back.at[slots(d)], sent_s.at[HOME], ret_r.at[k], (partner(d), j)
                )

    def home(g, which=None):
        if not which:
            red[g][0].wait_recv()
        for k in range(len(of(g))) if which is None else [which]:
            p = of(g)[k]
            r = bit(p)
            summed(g, k)
            done[r, :] = (
                part[0, r, :].astype(F32) + near[0, r, :].astype(F32) + far[r, :].astype(F32)
            ).astype(BF)
            for d in members(p):
                if d:
                    ret[d].start()
                else:
                    back[0:cap, :] = done[0:cap, :]

    for c in weight_loads:
        c.wait()
    arrive(0)
    down(0, gate_up(0, (0, 2, 1, 3)))
    forward(1, 0)
    forward(4)
    sums = gate_up(4, (0, 2))
    forward(1, 1)
    cross(0)
    arrive(4)
    down(4, gate_up(4, (1, 3), sums))
    sums = gate_up(1, (0,))
    cross(4)
    pair()
    arrive(1)
    sums = gate_up(1, (1,), sums)
    comb = sum(jnp.where(slot == target[t], rw_ref[t : t + 1, :], 0.0) for t in range(top)).T
    hi = comb.astype(BF)
    hi_ref[...] = hi
    lo_ref[...] = (comb - hi.astype(F32)).astype(BF)
    relay(1)
    sums = gate_up(1, (2,), sums)
    forward(3, 0)
    arrive(1, 1)
    down(1, gate_up(1, (3,), sums))
    forward(2)
    forward(3, 1)
    sums = gate_up(2, (0, 2))
    cross(1)
    arrive(2)
    sums = gate_up(2, (1, 3), sums)
    for r in range(1, rounds - 1):
        absorb(r)
    relay(3, 0)
    down(2, sums)
    arrive(3)
    sums = gate_up(3, (0,))
    relay(3, 1)
    sums = gate_up(3, (1,), sums)
    cross(2)
    sums = gate_up(3, (2,), sums)
    home(1, 0)
    arrive(3, 1)
    down(3, gate_up(3, (3,), sums))
    home(1, 1)
    home(0)
    cross(3)
    home(4)
    absorb(rounds - 1)
    retention()
    home(2)
    mix_cross()
    mix_c.start()
    home(3, 0)
    home(3, 1)

    def gather(k):
        ds = groups[k]
        r = (len(ds) - (0 in ds)) * cap
        send(count(r), count(r), sent_s.at[HOME], ret_r.at[k], (i, j1)).wait_recv()
        c = slice(position(ds[0]) * cap, position(ds[-1]) * cap + cap)
        return dot(hi_ref[:, c], back[c, :]) + dot(lo_ref[:, c], back[c, :])

    blend = gather(0) + gather(1) + gather(2)
    mix_a.wait_recv()
    mix_c.wait_recv()
    mixer_ref[...] = (
        mx[stripe(0), :].astype(F32) + mr1[0].astype(F32) + mr2[...].astype(F32)
    ).astype(BF)
    blend = blend + gather(3)
    expert_ref[...] = (blend + gather(4)).astype(BF)
    for kind, ref in (
        (DISPATCH, count((n - 1) * cap)), (BOTH, count((n // 2 - 1) * cap)), (ACROSS, count(rows // 2)),
        (CORE, x.at[pl.ds(0, 2)]), (HALVES, x.at[pl.ds(0, 2)]), (SUMS, count(rows)),
        (MIX, mx.at[pl.ds(0, 3 * quarter)]), (HOME, count((n - 1) * cap)),
    ):
        send(ref, ref, sent_s.at[kind], ret_r.at[0], (i, j1)).wait_send()
    st_c[0].wait_send()
    tot_c[0].wait_send()
    for r in range(1, rounds):
        @pl.when(i + (1 << r) < n)
        def _():
            st_c[r].wait_send()
            tot_c[r].wait_send()


def store_kernel(mixer, blended, mixer_out, blended_out, sem):
    copies = [
        pltpu.make_async_copy(mixer, mixer_out, sem.at[0]),
        pltpu.make_async_copy(blended, blended_out, sem.at[1]),
    ]
    for c in copies:
        c.start()
    for c in copies:
        c.wait()


def per_device(
    queries, key_rows, value_rows, out_gate, log_decay, head_gain, out_weight,
    moe_input, moe_gain, expert_gate, expert_up, expert_down, route_ids, route_weights,
):
    n, shares = lax.axis_size("ep"), lax.axis_size("tp")
    tokens, top = route_ids.shape
    pairs = tokens * top
    cap = -(-2 * pairs // n // 16) * 16
    full = moe_input.shape[1]
    width = full // shares
    length, heads = log_decay.shape
    dim = head_gain.shape[1]
    hidden = expert_gate.shape[2]

    rows = n * cap
    rounds = n.bit_length() - 1
    quarter = length // shares
    vmem = pl.BlockSpec(memory_space=pltpu.VMEM)
    hbm = pl.BlockSpec(memory_space=pltpu.HBM)
    dma = pltpu.SemaphoreType.DMA
    args = (
        moe_input, route_ids.T, moe_gain.reshape(1, full), log_decay.T, route_weights.T, head_gain,
        key_rows, value_rows, queries, out_gate, out_weight, expert_gate[0], expert_up[0], expert_down[0],
    )
    args = [pltpu.with_memory_space_constraint(a, pltpu.HBM) for a in args]
    mixer, blended = pl.pallas_call(
        functools.partial(layer_kernel, n, cap, heads),
        out_shape=(
            pltpu.VMEM((quarter, full), BF),
            pltpu.VMEM((tokens, width), BF),
        ),
        in_specs=[hbm] * len(args),
        out_specs=(vmem, vmem),
        scratch_shapes=[pltpu.VMEM(a.shape, a.dtype) for a in args[:6]] + [
            pltpu.VMEM((4, length, heads * dim), BF),
            pltpu.VMEM(out_weight.shape, BF),
            pltpu.VMEM((full, hidden), BF),
            pltpu.VMEM((full, hidden), BF),
            pltpu.VMEM((hidden, full), BF),
            pltpu.VMEM((4, rows, width), BF),
            pltpu.VMEM((4, rows, width), BF),
            pltpu.VMEM((2, rows, width), BF),
            pltpu.VMEM((rows, width), BF),
            pltpu.VMEM((rows, width), BF),
            pltpu.VMEM((rows, width), BF),
            pltpu.VMEM((rows, width), BF),
            pltpu.VMEM((rounds, heads * dim, dim), BF),
            pltpu.VMEM((rounds, heads * dim, dim), BF),
            pltpu.VMEM((rounds, 8, dim), F32),
            pltpu.VMEM((rounds, 8, dim), F32),
            pltpu.VMEM((heads * dim, dim), F32),
            pltpu.VMEM((heads * dim, dim), F32),
            pltpu.VMEM((length, heads * dim), F32),
            pltpu.VMEM((length, heads * dim), BF),
            pltpu.VMEM((length, full), BF),
            pltpu.VMEM((2, quarter, full), BF),
            pltpu.VMEM((quarter, full), BF),
            pltpu.VMEM((quarter, full), BF),
            dma((11,)), dma((8,)), dma((n - 1,)),
            dma((rounds,)), dma((rounds,)), dma((rounds,)), dma((rounds,)),
            dma((PIECES // 2,)), dma((7,)), dma((len(GROUPS), 2)), dma((7,)), dma((3,)), dma((5,)),
            pltpu.VMEM((rows, width), BF),
            pltpu.VMEM((rows, width), BF),
            pltpu.VMEM((tokens, rows), BF),
            pltpu.VMEM((tokens, rows), BF),
            pltpu.VMEM((length, heads * dim), BF),
            pltpu.VMEM((length, heads * dim), F32),
        ],
        compiler_params=pltpu.CompilerParams(
            collective_id=0, has_side_effects=True, vmem_limit_bytes=56 * 1024 * 1024
        ),
    )(*args)
    return pl.pallas_call(
        store_kernel,
        out_shape=(
            jax.ShapeDtypeStruct(mixer.shape, BF),
            jax.ShapeDtypeStruct(blended.shape, BF),
        ),
        in_specs=[vmem, vmem],
        out_specs=(hbm, hbm),
        scratch_shapes=[dma((2,))],
        compiler_params=pltpu.CompilerParams(vmem_limit_bytes=4 * 1024 * 1024),
    )(mixer, blended)


def solution(mesh):
    in_specs = (
        P("ep", "tp"),
        P("ep", "tp"),
        P("ep", "tp"),
        P("ep", "tp"),
        P("ep", "tp"),
        P("tp", None),
        P("tp", None),
        P("ep", None),
        P(),
        P("ep", None, "tp"),
        P("ep", None, "tp"),
        P("ep", "tp", None),
        P("ep", None),
        P("ep", None),
    )
    out_specs = (P(("ep", "tp"), None), P("ep", "tp"))
    return jax.shard_map(
        per_device, mesh=mesh, in_specs=in_specs, out_specs=out_specs, check_vma=False
    )
```
